256 devices in a mesh: sp: 32 (over z, y), tp: 8 (over x, core).
Axes of the slice: x: 4, y: 4, z: 8, core: 2. Of those that a mesh axis runs over, the one named last changes fastest.
Arguments:
- block_input: bfloat16 [32768, 2048], P('sp'), may hold values from -6 to 6
- value_proj: bfloat16 [2048, 1024], P(None, 'tp'), may hold values from -0.125 to 0.125
- gate_proj: bfloat16 [2048, 1024], P(None, 'tp'), may hold values from -0.125 to 0.125
- conv_taps: float32 [31, 1024], P(None, 'tp'), may hold values from -3 to 3
- norm_gain: float32 [1024], P('tp'), may hold values from 0.1 to 1.9
- out_proj: bfloat16 [2048, 1024], P(None, 'tp'), may hold values from -0.125 to 0.125
- grad_output: bfloat16 [32768, 2048], P('sp'), may hold values from -6 to 6
Outputs:
- input_grad: bfloat16 [32768, 2048], P('sp', 'tp')
- value_grad: float32 [2048, 1024], P('sp', 'tp')
- gate_grad: float32 [2048, 1024], P('sp', 'tp')
- out_grad: float32 [2048, 1024], P('sp', 'tp')
- taps_grad: float32 [31, 1024], P(None, 'tp')
- gain_grad: float32 [1024], P('tp')
The draws below stay inside these ranges and needn't reach their ends.
All inputs are finite; a program needn't handle non-finite values.
Results may differ from the reference program's by a relative error of at most 0.015.
Values may be sent and summed in bfloat16 or wider, within the bound.
A program may use at most 64 MiB of HBM per device.

```python
import jax
import jax.numpy as jnp
from jax import lax

D = 2048
C = 1024
K = 31
TOKENS = 32768
N_TP = 8


def draw_conv_taps(key, part):
    base_key, order_key = jax.random.split(key)
    raw_taps = jnp.clip(jax.random.normal(base_key, (K, C), jnp.float32), -4.0, 4.0)
    group_order = jax.random.permutation(order_key, 8).astype(jnp.float32)
    group_index = jnp.arange(C) * 8 // C
    group_scale = 0.3 * 10.0 ** (group_order[group_index] / 7.0)
    return raw_taps * group_scale[None, :] / jnp.sqrt(jnp.float32(K))


def with_spikes(result, key, source, target, blocks, factor):
    def block_of(dim):
        return (jnp.arange(result.shape[dim]) // (result.shape[dim] // blocks)).reshape((-1,) + (1,) * (result.ndim - 1 - dim))

    one_side = jax.random.permutation(key, blocks)[block_of(target)]
    far = (block_of(target) + blocks // 2) % blocks
    return jnp.where((block_of(source) == one_side) | (block_of(source) == far), factor * result, result)


def block_scale(stream_key, shape, cuts, least, high):
    def one(axis_at, parts):
        heights = jax.random.uniform(jax.random.fold_in(jax.random.fold_in(stream_key, 6), axis_at), (parts,), jnp.float32, least / len(cuts), high / len(cuts))
        return jnp.repeat(jnp.exp(heights), shape[axis_at] // parts).reshape((-1,) + (1,) * (len(shape) - axis_at - 1))

    loudness = one(*cuts[0])
    for cut in cuts[1:]:
        loudness = loudness * one(*cut)
    return loudness


def normal_values(stream_key, dims, spread, reach, cuts=(), dtype=jnp.bfloat16):
    values = spread * jax.random.normal(stream_key, dims, jnp.float32)
    if cuts:
        values = values * block_scale(stream_key, dims, cuts, -0.22, 0.18)
    return jnp.clip(values, -reach, reach).astype(dtype)


def bell_draw_with(rng, shape, deviation, most, pieces, heavy, held_as=jnp.bfloat16):
    entries = deviation * jax.random.normal(rng, shape, jnp.float32)
    if pieces:
        entries = entries * block_scale(rng, shape, pieces, -0.22, 0.18)
    return jnp.clip(with_spikes(entries, jax.random.fold_in(rng, 3), *heavy), -most, most).astype(held_as)


def setup_inputs(seed: int = 0) -> dict:
    keys = jax.random.split(jax.random.key(seed), 8)
    block_input = bell_draw_with(keys[0], (TOKENS, D), 1.0, 6.0, ((0, 32),), (0, 1, 32, 2.75))
    value_proj = normal_values(keys[1], (D, C), D ** -0.5, 0.125, ((1, 8),))
    gate_proj = normal_values(keys[2], (D, C), D ** -0.5, 0.125, ((1, 8),))
    conv_taps = draw_conv_taps(jax.random.fold_in(keys[7], 71), 0)
    norm_gain = jnp.clip(1.0 + 0.18 * jax.random.normal(keys[4], (C,), jnp.float32), 0.1, 1.9)
    out_proj = normal_values(keys[5], (D, C), D ** -0.5, 0.125, ((1, 8),))
    grad_output = bell_draw_with(keys[6], (TOKENS, D), 1.0, 6.0, ((0, 32),), (0, 1, 32, 2.75))
    return dict(block_input=block_input, value_proj=value_proj, gate_proj=gate_proj, conv_taps=conv_taps, norm_gain=norm_gain, out_proj=out_proj, grad_output=grad_output)


norm_floor = 0.1

def reference(block_input, value_proj, gate_proj, conv_taps, norm_gain, out_proj, grad_output):
    value = jnp.dot(block_input, value_proj, preferred_element_type=jnp.float32)
    gate_raw = jnp.dot(block_input, gate_proj, preferred_element_type=jnp.float32)
    sgate = jax.nn.sigmoid(gate_raw)
    mixed = (value * sgate).astype(jnp.bfloat16)
    tap_count = conv_taps.shape[0]
    reach_rows = tap_count - 1
    seq_rows = mixed.shape[0]
    history = jnp.concatenate([jnp.zeros((reach_rows, C), jnp.bfloat16), mixed], axis=0)
    conv_out = jnp.zeros((seq_rows, C), jnp.float32)
    for tap_index in range(tap_count):
        offset = reach_rows - tap_index
        conv_out = conv_out + conv_taps[tap_index] * history[offset:offset + seq_rows].astype(jnp.float32)
    center = lax.optimization_barrier(jnp.sum(conv_out, axis=1)) / C
    squares = lax.optimization_barrier(jnp.sum(conv_out * conv_out, axis=1)) / C
    inverse = lax.rsqrt(squares - center * center + norm_floor)
    normed = (conv_out - center[:, None]) * inverse[:, None]
    scaled = normed * norm_gain
    squash = jax.nn.sigmoid(scaled)
    activated = (scaled * squash).astype(jnp.bfloat16)
    slope = jnp.dot(grad_output, out_proj, preferred_element_type=jnp.float32)
    pre_slope = slope * squash * (1.0 + scaled * (1.0 - squash))
    gain_grad = lax.optimization_barrier(jnp.sum(pre_slope * normed, axis=0))
    norm_slope = pre_slope * norm_gain
    slope_sum = lax.optimization_barrier(jnp.sum(norm_slope, axis=1)) / C
    cross_sum = lax.optimization_barrier(jnp.sum(norm_slope * normed, axis=1)) / C
    conv_slope = inverse[:, None] * (norm_slope - slope_sum[:, None] - normed * cross_sum[:, None])
    taps_list = []
    for tap_index in range(tap_count):
        offset = reach_rows - tap_index
        taps_list.append(lax.optimization_barrier(jnp.sum(conv_slope * history[offset:offset + seq_rows].astype(jnp.float32), axis=0)))
    taps_grad = jnp.stack(taps_list)
    future = jnp.concatenate([conv_slope, jnp.zeros((reach_rows, C), jnp.float32)], axis=0)
    mixed_slope = jnp.zeros((seq_rows, C), jnp.float32)
    for tap_index in range(tap_count):
        mixed_slope = mixed_slope + conv_taps[tap_index] * future[tap_index:tap_index + seq_rows]
    value_slope = (mixed_slope * sgate).astype(jnp.bfloat16)
    gate_slope = (mixed_slope * value * sgate * (1.0 - sgate)).astype(jnp.bfloat16)
    value_grad = jnp.dot(block_input.T, value_slope, preferred_element_type=jnp.float32)
    gate_grad = jnp.dot(block_input.T, gate_slope, preferred_element_type=jnp.float32)
    out_grad = jnp.dot(grad_output.T, activated, preferred_element_type=jnp.float32)
    group_width = C // N_TP
    running = jnp.zeros((seq_rows, D), jnp.float32)
    for group_index in range(N_TP):
        first_col = group_index * group_width
        last_col = first_col + group_width
        partial_value = jnp.dot(value_slope[:, first_col:last_col], value_proj[:, first_col:last_col].T, preferred_element_type=jnp.float32)
        partial_value = partial_value + jnp.dot(gate_slope[:, first_col:last_col], gate_proj[:, first_col:last_col].T, preferred_element_type=jnp.float32)
        rounded = lax.optimization_barrier(partial_value.astype(jnp.bfloat16))
        running = running + rounded.astype(jnp.float32)
    input_grad = running.astype(jnp.bfloat16)
    return (input_grad, value_grad, gate_grad, out_grad, taps_grad, gain_grad)
```

```python
import functools

import jax
import jax.numpy as jnp
from jax import lax
from jax.experimental import pallas as pl
from jax.experimental.pallas import tpu as pltpu
from jax.sharding import Mesh
from jax.sharding import PartitionSpec as P

MESH = pl.DeviceIdType.MESH
F32 = jnp.float32
BF16 = jnp.bfloat16
norm_floor = 0.1
L = 128
S = 8
J = 8
PAD = 32
NC = 4


def dot_nn(a, b):
    return lax.dot_general(a, b, (((1,), (0,)), ((), ())), preferred_element_type=F32)


def dot_nt(a, b):
    return lax.dot_general(a, b, (((1,), (1,)), ((), ())), preferred_element_type=F32)


def body(
    Z, Y, C, K,
    x_hbm, vp_hbm, gp_hbm, taps, gain, op_hbm, g_hbm,
    ig, vg, gg, og, tg, ng,
    xv, gv, wvg, wo, wg, vbuf, sbuf, slope, hist, convp, nrm, nsl, act, cs, vsf, gsf, sl, slg, acc,
    actT, slT, wgo, wgv, yro, yrv, zso, zsv, zro, zrv, sta, star, stb, stbr, tgs, tgy, tgzs, tgz,
    l_sem, x_sem, g_sem, w_ss, w_rs, h_ss, h_rs, sa_ss, sa_rs, sb_ss, sb_rs, own_ss, fwd_ss, pf_ss, slg_rs,
    yo_ss, yo_rs, yv_ss, yv_rs, zo_ss, zo_rs, zv_ss, zv_rs, ty_ss, ty_rs, tz_ss, tz_rs, ow_sem,
):
    z, y, x, c = (lax.axis_index(a) for a in ("z", "y", "x", "c"))
    rows, D = xv.shape
    T = rows // S
    DB = D // 8
    RB = D // (Z * Y)
    CH = rows // NC
    H = K - 1

    yn = (y + 1) % Y
    zn = (z + (y + 1) // Y) % Z
    yb = (y + Y - 1) % Y
    zb = (z + Z - 1 + (y + Y - 1) // Y) % Z
    first = (z + y) == 0
    last = (z * Y + y) == (Z * Y - 1)
    xp, xm = (x + 1) % 4, (x + 3) % 4
    xs = (x, x + 1 - 2 * (x % 2), (x + 2) % 4, 3 - x)
    cc = (c, 1 - c)

    def to(z=z, y=y, x=x, c=c):
        return {"z": z, "y": y, "x": x, "c": c}

    def remote(src, dst, ss, rs, dev):
        return pltpu.make_async_remote_copy(
            src_ref=src, dst_ref=dst, send_sem=ss, recv_sem=rs, device_id=dev, device_id_type=MESH
        )

    tp_peers = [to(x=xs[o // 2], c=cc[o % 2]) for o in range(1, 8)]
    y_peers = [to(y=(y + d) % Y) for d in range(1, Y)]
    z_peers = [to(z=(z + d) % Z) for d in range(1, Z)]
    nxt, prv = to(z=zn, y=yn), to(z=zb, y=yb)
    sent = []

    loads = [
        pltpu.make_async_copy(vp_hbm, wvg.at[:, pl.ds(0, L)], l_sem.at[0]),
        pltpu.make_async_copy(gp_hbm, wvg.at[:, pl.ds(L, L)], l_sem.at[1]),
        pltpu.make_async_copy(op_hbm, wo, l_sem.at[2]),
    ]
    loads[0].start()
    loads[1].start()
    XC = 4
    XR = rows // XC

    def x_load(i):
        at = pl.ds(pl.multiple_of(i * XR, XR), XR)
        return pltpu.make_async_copy(x_hbm.at[at], xv.at[at], x_sem.at[i])

    def g_load(i):
        at = pl.ds(pl.multiple_of(i * XR, XR), XR)
        return pltpu.make_async_copy(g_hbm.at[at], gv.at[at], g_sem.at[i])

    for i in (XC - 1, *range(XC - 1)):
        x_load(i).start()
    loads[2].start()
    for i in range(XC):
        g_load(i).start()

    barrier = pltpu.get_barrier_semaphore()
    greet = [*tp_peers, *y_peers, *z_peers, nxt, prv]
    for dev in greet:
        pl.semaphore_signal(barrier, inc=1, device_id=dev, device_id_type=MESH)
    pl.semaphore_wait(barrier, len(greet))

    loads[0].wait()
    loads[1].wait()

    w_copies = []
    for o in range(1, 8):
        px, pc = xs[o // 2], cc[o % 2]
        at = pl.ds(pl.multiple_of((px * 2 + pc) * DB, DB), DB)
        w_copies.append(remote(wvg.at[at], wg.at[o - 1], w_ss.at[o - 1], w_rs.at[o - 1], tp_peers[o - 1]))
    for cp in w_copies:
        cp.start()

    def x_step(i):
        x_load(i).wait()
        at = pl.ds(pl.multiple_of(i * XR, XR), XR)
        res = dot_nn(xv[at, :], wvg[...])
        v = res[:, :L]
        s = jax.nn.sigmoid(res[:, L:])
        vbuf[at, :] = v
        sbuf[at, :] = s
        hist[pl.ds(pl.multiple_of(PAD + i * XR, PAD), XR), :] = (v * s).astype(BF16).astype(F32)

    x_step(XC - 1)
    halo_m = remote(hist.at[pl.ds(rows, PAD)], hist.at[pl.ds(0, PAD)], h_ss.at[0], h_rs.at[0], nxt)
    halo_m.start()

    def x_loop(i, carry):
        x_step(i)
        return carry

    lax.fori_loop(0, XC - 1, x_loop, 0)
    loads[2].wait()

    def g_loop(i, carry):
        g_load(i).wait()
        at = pl.ds(pl.multiple_of(i * XR, XR), XR)
        slope[at, :] = dot_nn(gv[at, :], wo[...])
        return carry

    lax.fori_loop(0, XC, g_loop, 0)

    halo_m.wait_recv()

    @pl.when(first)
    def _():
        hist[pl.ds(0, PAD), :] = jnp.zeros((PAD, L), F32)

    lane = lax.broadcasted_iota(jnp.int32, (S, L), 1)
    zero = jnp.zeros((S, L), F32)

    def rows_of(ref, t):
        return ref[pl.ds(t, S, stride=T), :]

    def spread(stat, t):
        return jnp.sum(jnp.where(lane == t, stat, 0.0), axis=1, keepdims=True)

    def tap(k):
        return taps[pl.ds(k, 1), :]

    def conv_block(b, carry):
        s1, s2 = carry
        t0 = b * J
        m = [rows_of(hist, t0 + (PAD - H) + i) for i in range(J + H)]
        for j in range(J):
            r = tap(0) * m[H + j]
            for k in range(1, K):
                r = r + tap(k) * m[H + j - k]
            convp[t0 + j] = r
            s1 = jnp.where(lane == t0 + j, jnp.sum(r, axis=1, keepdims=True), s1)
            s2 = jnp.where(lane == t0 + j, jnp.sum(r * r, axis=1, keepdims=True), s2)
        return s1, s2

    def exchange(own, got, ss, rs):
        copies = [remote(own, got.at[i], ss.at[i], rs.at[i], tp_peers[i]) for i in range(7)]
        for cp in copies:
            cp.start()
        sent.extend(copies)
        return copies

    def total(own, got, i):
        r = own[i]
        for p in range(7):
            r = r + got[p, i]
        return r * (1.0 / C)

    s1, s2 = lax.fori_loop(0, T // J, conv_block, (zero, zero))
    sta[0] = s1
    sta[1] = s2
    ex = exchange(sta, star, sa_ss, sa_rs)
    for cp in ex:
        cp.wait_recv()
    center = total(sta, star, 0)
    inverse = lax.rsqrt(total(sta, star, 1) - center * center + norm_floor)
    gains = gain[...]

    def norm_block(b, carry):
        gsum, s1, s2 = carry
        t0 = b * J
        for j in range(J):
            t = t0 + j
            n = (convp[t] - spread(center, t)) * spread(inverse, t)
            sc = n * gains
            sq = jax.nn.sigmoid(sc)
            act[pl.ds(t, S, stride=T), :] = sc * sq
            ps = rows_of(slope, t) * sq * (1.0 + sc * (1.0 - sq))
            gsum = gsum + ps * n
            ns = ps * gains
            nrm[t] = n
            nsl[t] = ns
            s1 = jnp.where(lane == t, jnp.sum(ns, axis=1, keepdims=True), s1)
            s2 = jnp.where(lane == t, jnp.sum(ns * n, axis=1, keepdims=True), s2)
        return gsum, s1, s2

    gsum, s1, s2 = lax.fori_loop(0, T // J, norm_block, (zero, zero, zero))
    stb[0] = s1
    stb[1] = s2
    ex = exchange(stb, stbr, sb_ss, sb_rs)

    def flip(src, dst, row0):
        def step(i, carry):
            at = pl.multiple_of(i * L, L)
            dst[pl.ds(row0, L), pl.ds(at, L)] = src[pl.ds(at, L), :].T.astype(BF16)
            return carry

        lax.fori_loop(0, rows // L, step, 0)

    flip(act, actT, 0)

    def weight_grad(left, right, dst):
        def step(zi, carry):
            at = pl.ds(pl.multiple_of(zi * (D // Z), D // Z), D // Z)
            r = dot_nn(left[...], right[:, at]).T.astype(BF16)
            for yi in range(Y):
                dst[zi, yi] = r[yi * RB : (yi + 1) * RB, :]
            return carry

        lax.fori_loop(0, Z, step, 0)

    def y_send(src, dst, ss, rs):
        copies = []
        for d in range(1, Y):
            copies.append(
                remote(src.at[:, (y + d) % Y], dst.at[d - 1], ss.at[d - 1], rs.at[d - 1], y_peers[d - 1])
            )
            copies[-1].start()
        sent.extend(copies)
        return copies

    weight_grad(actT, gv, wgo)
    yo = y_send(wgo, yro, yo_ss, yo_rs)

    for cp in ex:
        cp.wait_recv()
    slope_sum = total(stb, stbr, 0)
    cross_sum = total(stb, stbr, 1)

    def cs_block(b, carry):
        t0 = b * J
        for j in range(J):
            t = t0 + j
            cs[pl.ds(t, S, stride=T), :] = spread(inverse, t) * (
                nsl[t] - spread(slope_sum, t) - nrm[t] * spread(cross_sum, t)
            )
        return carry

    lax.fori_loop(0, PAD // J, cs_block, 0)
    halo_c = remote(cs.at[pl.ds(0, PAD)], cs.at[pl.ds(rows, PAD)], h_ss.at[1], h_rs.at[1], prv)
    halo_c.start()
    lax.fori_loop(PAD // J, T // J, cs_block, 0)

    def tap_block(b, sums):
        sums = list(sums)
        t0 = b * J
        m = [rows_of(hist, t0 + (PAD - H) + i) for i in range(J + H)]
        for j in range(J):
            e = rows_of(cs, t0 + j)
            for k in range(K):
                sums[k] = sums[k] + e * m[H + j - k]
        return tuple(sums)

    sums = lax.fori_loop(0, T // J, tap_block, tuple(zero for _ in range(K)))
    for k in range(K):
        tgs[pl.ds(k, 1), :] = jnp.sum(sums[k], axis=0, keepdims=True)
    tgs[pl.ds(K, 1), :] = jnp.sum(gsum, axis=0, keepdims=True)
    ty = []
    for d in range(1, Y):
        ty.append(remote(tgs, tgy.at[y], ty_ss.at[d - 1], ty_rs.at[d - 1], y_peers[d - 1]))
        ty[-1].start()
    sent.extend(ty)
    tgy[y] = tgs[...]

    halo_c.wait_recv()

    @pl.when(last)
    def _():
        cs[pl.ds(rows, PAD), :] = jnp.zeros((PAD, L), F32)

    def slope_block(b, carry):
        t0 = b * J
        f = [rows_of(cs, t0 + i) for i in range(J + H)]
        for j in range(J):
            t = t0 + j
            r = tap(0) * f[j]
            for k in range(1, K):
                r = r + tap(k) * f[j + k]
            s = rows_of(sbuf, t)
            rs = r * s
            vsf[pl.ds(t, S, stride=T), :] = rs
            gsf[pl.ds(t, S, stride=T), :] = rs * rows_of(vbuf, t) * (1.0 - s)
        return carry

    lax.fori_loop(0, T // J, slope_block, 0)
    sl[:, pl.ds(0, L)] = vsf[...].astype(BF16)
    sl[:, pl.ds(L, L)] = gsf[...].astype(BF16)

    def piece(ref, q):
        return ref.at[pl.ds(q * CH, CH)]

    def own_copy(way, slot, q, dev):
        return remote(piece(sl, q), piece(slg.at[slot], q), own_ss.at[way, q], slg_rs.at[slot, q], dev)

    right, left = to(x=xp), to(x=xm)
    partner = to(c=1 - c)
    up = [own_copy(0, 1, q, right) for q in range(NC)]
    down = [own_copy(1, 2, q, left) for q in range(NC)]
    over = [own_copy(2, 0, q, partner) for q in range(NC)]
    half = NC // 2
    for i in range(NC):
        up[i].start()
        down[(i + half) % NC].start()
    for i in range(NC):
        over[i].start()
    sent.extend([*up, *down, *over])

    flip(vsf, slT, 0)
    flip(gsf, slT, L)
    weight_grad(slT, xv, wgv)
    yv = y_send(wgv, yrv, yv_ss, yv_rs)

    for cp in w_copies:
        cp.wait_recv()
    sent.extend(w_copies)

    def weights_from(slot):
        core = 1 if slot == 0 or slot > 3 else 0
        base = slot if slot <= 3 else slot - 3
        if base == 0:
            return wg[0]
        if base == 3:
            return wg[3 + core]
        way = 3 - 2 * (x % 2) if base == 1 else 1 + 2 * (x % 2)
        return wg[2 * way + core - 1]

    at = pl.ds(pl.multiple_of((x * 2 + c) * DB, DB), DB)
    acc[...] = dot_nt(sl[...], wvg[at, :])

    def add(slot, q):
        at = pl.ds(q * CH, CH)
        acc[at, :] += dot_nt(slg[slot, at, :], weights_from(slot))

    def pf(slot, q):
        cp = remote(
            piece(slg.at[slot], q), piece(slg.at[slot + 3], q), pf_ss.at[slot - 1, q], slg_rs.at[slot + 3, q], partner
        )
        cp.start()
        sent.append(cp)
        return cp

    fwd = {}
    pfs = {}
    for i in range(NC):
        q = i
        up[q].wait_recv()
        if i < half:
            fwd[q] = remote(piece(slg.at[1], q), piece(slg.at[3], q), fwd_ss.at[q], slg_rs.at[3, q], right)
            fwd[q].start()
        pfs[1, q] = pf(1, q)
        q2 = (i + half) % NC
        down[q2].wait_recv()
        if i < half:
            fwd[q2] = remote(piece(slg.at[2], q2), piece(slg.at[3], q2), fwd_ss.at[q2], slg_rs.at[3, q2], left)
            fwd[q2].start()
        pfs[2, q2] = pf(2, q2)
        over[i].wait_recv()
        add(0, i)
        add(1, q)
        add(2, q2)
        if i == 2:
            for cp in yo:
                cp.wait_recv()
            zo = second(Z, Y, y, z, wgo, yro, zso, zro, zo_ss, zo_rs, z_peers, remote, sent)
            for cp in ty:
                cp.wait_recv()
            t = tgy[0]
            for yi in range(1, Y):
                t = t + tgy[yi]
            tgzs[...] = t
            tgz[z] = t
            tz = []
            for d in range(1, Z):
                tz.append(remote(tgzs, tgz.at[z], tz_ss.at[d - 1], tz_rs.at[d - 1], z_peers[d - 1]))
                tz[-1].start()
            sent.extend(tz)
    sent.extend(fwd.values())
    for i in range(NC):
        add_q = i
        pfs[1, add_q].wait_recv()
        add(4, add_q)
        pfs[2, add_q].wait_recv()
        add(5, add_q)

    for cp in yv:
        cp.wait_recv()
    zv = second(Z, Y, y, z, wgv, yrv, zsv, zrv, zv_ss, zv_rs, z_peers, remote, sent)

    order = [q for i in range(half) for q in (i, i + half)]
    for q in order:
        fwd[q].wait_recv()
        pfs[3, q] = pf(3, q)
        add(3, q)
    for q in order:
        pfs[3, q].wait_recv()
        add(6, q)
    ig[...] = acc[...].astype(BF16)

    for cp in zo:
        cp.wait_recv()
    r = zso[z].astype(F32)
    for d in range(1, Z):
        r = r + zro[d - 1].astype(F32)
    og[...] = r
    for cp in tz:
        cp.wait_recv()
    t = tgz[0]
    for zi in range(1, Z):
        t = t + tgz[zi]
    tg[...] = t[:K]
    ng[...] = t[K : K + 1]
    for cp in zv:
        cp.wait_recv()
    r = zsv[z].astype(F32)
    for d in range(1, Z):
        r = r + zrv[d - 1].astype(F32)
    vg[...] = r[:, :L]
    gg[...] = r[:, L:]

    for cp in [halo_m, halo_c, *sent]:
        cp.wait_send()


def second(Z, Y, y, z, own, got, zs, zr, ss, rs, z_peers, remote, sent):
    def step(zi, carry):
        r = own[zi, y].astype(F32)
        for d in range(Y - 1):
            r = r + got[d, zi].astype(F32)
        zs[zi] = r.astype(BF16)
        return carry

    lax.fori_loop(0, Z, step, 0)
    copies = []
    for d in range(1, Z):
        copies.append(remote(zs.at[(z + d) % Z], zr.at[d - 1], ss.at[d - 1], rs.at[d - 1], z_peers[d - 1]))
        copies[-1].start()
    sent.extend(copies)
    return copies


def shards(Z, Y, block_input, value_proj, gate_proj, conv_taps, norm_gain, out_proj, grad_output):
    rows, D = block_input.shape
    K = conv_taps.shape[0]
    C = value_proj.shape[1] * 8
    DB, RB, T = D // 8, D // (Z * Y), rows // S
    vm = pltpu.VMEM
    dma = pltpu.SemaphoreType.DMA
    any_, vmem = pl.BlockSpec(memory_space=pl.ANY), pl.BlockSpec(memory_space=pltpu.VMEM)
    scratch = [
        vm((rows, D), BF16), vm((rows, D), BF16), vm((D, 2 * L), BF16), vm((D, L), BF16), vm((7, DB, 2 * L), BF16),
        vm((rows, L), F32), vm((rows, L), F32), vm((rows, L), F32), vm((rows + PAD, L), F32),
        vm((T, S, L), F32), vm((T, S, L), F32), vm((T, S, L), F32), vm((rows, L), F32), vm((rows + PAD, L), F32),
        vm((rows, L), F32), vm((rows, L), F32), vm((rows, 2 * L), BF16), vm((7, rows, 2 * L), BF16), vm((rows, DB), F32),
        vm((L, rows), BF16), vm((2 * L, rows), BF16),
        vm((Z, Y, RB, L), BF16), vm((Z, Y, RB, 2 * L), BF16),
        vm((Y - 1, Z, RB, L), BF16), vm((Y - 1, Z, RB, 2 * L), BF16),
        vm((Z, RB, L), BF16), vm((Z, RB, 2 * L), BF16), vm((Z - 1, RB, L), BF16), vm((Z - 1, RB, 2 * L), BF16),
        vm((2, S, L), F32), vm((7, 2, S, L), F32), vm((2, S, L), F32), vm((7, 2, S, L), F32),
        vm((PAD, L), F32), vm((Y, PAD, L), F32), vm((PAD, L), F32), vm((Z, PAD, L), F32),
        dma((3,)), dma((4,)), dma((4,)), dma((7,)), dma((7,)), dma((2,)), dma((2,)),
        dma((7,)), dma((7,)), dma((7,)), dma((7,)), dma((3, NC)), dma((NC,)), dma((3, NC)), dma((7, NC)),
        *[dma((Y - 1,)) for _ in range(4)], *[dma((Z - 1,)) for _ in range(4)],
        dma((Y - 1,)), dma((Y - 1,)), dma((Z - 1,)), dma((Z - 1,)), dma((1,)),
    ]
    outs = pl.pallas_call(
        functools.partial(body, Z, Y, C, K),
        out_shape=(
            jax.ShapeDtypeStruct((rows, DB), BF16),
            jax.ShapeDtypeStruct((RB, L), F32),
            jax.ShapeDtypeStruct((RB, L), F32),
            jax.ShapeDtypeStruct((RB, L), F32),
            jax.ShapeDtypeStruct((K, L), F32),
            jax.ShapeDtypeStruct((1, L), F32),
        ),
        in_specs=[any_, any_, any_, vmem, vmem, any_, any_],
        out_specs=[vmem] * 6,
        scratch_shapes=scratch,
        compiler_params=pltpu.CompilerParams(
            collective_id=0, has_side_effects=True, vmem_limit_bytes=56 * 1024 * 1024
        ),
        name="block_backward",
    )(block_input, value_proj, gate_proj, conv_taps, norm_gain.reshape(1, L), out_proj, grad_output)
    return (*outs[:5], outs[5].reshape(L))


def solution(mesh):
    tp = mesh.shape["tp"]
    Y = 4
    Z = mesh.shape["sp"] // Y
    finer = Mesh(mesh.devices.reshape(Z, Y, tp // 2, 2), ("z", "y", "x", "c"))
    sp, ch = ("z", "y"), ("x", "c")
    return jax.shard_map(
        functools.partial(shards, Z, Y),
        mesh=finer,
        in_specs=(P(sp, None), P(None, ch), P(None, ch), P(None, ch), P(ch), P(None, ch), P(sp, None)),
        out_specs=(P(sp, ch), P(sp, ch), P(sp, ch), P(sp, ch), P(None, ch), P(ch)),
        check_vma=False,
    )
```

```python
import functools

import jax
import jax.numpy as jnp
from jax import lax
from jax.experimental import pallas as pl
from jax.experimental.pallas import tpu as pltpu
from jax.sharding import Mesh
from jax.sharding import PartitionSpec as P

MESH = pl.DeviceIdType.MESH
F32 = jnp.float32
BF16 = jnp.bfloat16
norm_floor = 0.1
ANYWHERE = pltpu.HBM
VMEM_LIMIT = 40 * 1024 * 1024
L = 128
S = 8
J = 16
NP = 132
HP = 164
PAD = 32
NC = 4


def dot_nn(a, b):
    return lax.dot_general(a, b, (((1,), (0,)), ((), ())), preferred_element_type=F32)


def dot_nt(a, b):
    return lax.dot_general(a, b, (((1,), (1,)), ((), ())), preferred_element_type=F32)


def body(
    Z, Y, C, K,
    x_hbm, vp_hbm, gp_hbm, taps, gain, op_hbm, g_hbm,
    ig, vg, gg, og, tg, ng,
    xv, gv, wvg, wo, wg, vbuf, sbuf, slope, hist, convp, nrm, nsl, inv, act, cs, vsf, gsf, sl, slg, acc,
    tail, halo_in, halo_out, halo_back,
    actT, slT, wgo, wgv, wgg, yro, yrv, zso, zsv, zro, zrv, zrg, ysg, yrg, sta, star, stb, stbr, tgs, tgy, tgzs, tgz,
    l_sem, x_sem, g_sem, wo_ss, wo_rs, w_ss, w_rs, wy_ss, wy_rs, h_ss, h_rs, sa_ss, sa_rs, sb_ss, sb_rs, own_ss, fwd_ss, pf_ss, slg_rs,
    yo_ss, yo_rs, yv_ss, yv_rs, yg_ss, yg_rs, zo_ss, zo_rs, zv_ss, zv_rs, zg_ss, zg_rs, ty_ss, ty_rs, tz_ss, tz_rs,
):
    z, y, x, c = (lax.axis_index(a) for a in ("z", "y", "x", "c"))
    rows, D = xv.shape
    T = rows // S
    DB = D // 8
    DQ = DB // 4
    RB = D // (Z * Y)
    CH = rows // NC
    H = K - 1

    yn = (y + 1) % Y
    zn = (z + (y + 1) // Y) % Z
    yb = (y + Y - 1) % Y
    zb = (z + Z - 1 + (y + Y - 1) // Y) % Z
    first = (z + y) == 0
    last = (z * Y + y) == (Z * Y - 1)
    xp, xm = (x + 1) % 4, (x + 3) % 4
    xs = (x, x + 1 - 2 * (x % 2), (x + 2) % 4, 3 - x)
    cc = (c, 1 - c)

    def to(z=z, y=y, x=x, c=c):
        return {"z": z, "y": y, "x": x, "c": c}

    def remote(src, dst, ss, rs, dev):
        return pltpu.make_async_remote_copy(
            src_ref=src, dst_ref=dst, send_sem=ss, recv_sem=rs, device_id=dev, device_id_type=MESH
        )

    tp_peers = [to(x=xs[o // 2], c=cc[o % 2]) for o in range(1, 8)]
    y_peers = [to(y=(y + d) % Y) for d in range(1, Y)]
    z_peers = [to(z=(z + d) % Z) for d in range(1, Z)]
    nxt, prv = to(z=zn, y=yn), to(z=zb, y=yb)
    sent = []

    loads = [
        pltpu.make_async_copy(vp_hbm, wvg.at[:, pl.ds(0, L)], l_sem.at[0]),
        pltpu.make_async_copy(gp_hbm, wvg.at[:, pl.ds(L, L)], l_sem.at[1]),
        pltpu.make_async_copy(op_hbm, wo, l_sem.at[2]),
    ]
    loads[0].start()
    loads[1].start()
    XC = 4
    XR = rows // XC

    def x_load(i):
        at = pl.ds(pl.multiple_of(i * XR, XR), XR)
        return pltpu.make_async_copy(x_hbm.at[at], xv.at[at], x_sem.at[i])

    def g_load(i):
        at = pl.ds(pl.multiple_of(i * XR, XR), XR)
        return pltpu.make_async_copy(g_hbm.at[at], gv.at[at], g_sem.at[i])

    for i in (XC - 1, *range(XC - 1)):
        x_load(i).start()
    loads[2].start()
    for i in range(XC):
        g_load(i).start()

    barrier = pltpu.get_barrier_semaphore()
    greet = [*tp_peers, *y_peers, *z_peers, nxt, prv]
    for dev in greet:
        pl.semaphore_signal(barrier, inc=1, device_id=dev, device_id_type=MESH)

    loads[0].wait()
    loads[1].wait()

    def x_step(i, end):
        x_load(i).wait()
        res = dot_nn(xv[pl.ds(pl.multiple_of(i * XR, XR), XR), :], wvg[...])
        v = res[:, :L]
        s = jax.nn.sigmoid(res[:, L:])
        m = (v * s).astype(BF16).astype(F32)
        for h in range(XR // T):
            n = i * (XR // T) + h
            part = slice(h * T, (h + 1) * T)
            vbuf[pl.ds(n * NP, T), :] = v[part]
            sbuf[pl.ds(n * NP, T), :] = s[part]
            hist[pl.ds(n * HP + PAD, T), :] = m[part]
            if end and h == XR // T - 1:
                tail[...] = m[XR - PAD :]
            else:
                hist[pl.ds((n + 1) * HP, PAD), :] = m[(h + 1) * T - PAD : (h + 1) * T]

    x_step(XC - 1, True)

    def x_loop(i, carry):
        x_step(i, False)
        return carry

    lax.fori_loop(0, XC - 1, x_loop, 0)

    pl.semaphore_wait(barrier, len(greet))
    halo_m = remote(tail, halo_in, h_ss.at[0], h_rs.at[0], nxt)
    halo_m.start()

    yq, zq = y % 2, z % 2
    w_copies, w_own = [], []
    for o in range(1, 8):
        px, pc = xs[o // 2], cc[o % 2]
        row = (px * 2 + pc) * DB
        if o == 1:
            for i in range(4):
                at = pl.ds(pl.multiple_of(row + i * DQ, DQ), DQ)
                w_own.append(remote(wvg.at[at], wg.at[0, i // 2, i % 2], wo_ss.at[i], wo_rs.at[i], tp_peers[0]))
                w_own[-1].start()
        else:
            at = pl.ds(pl.multiple_of(row + (2 * yq + zq) * DQ, DQ), DQ)
            w_copies.append(
                remote(wvg.at[at], wg.at[o - 1, yq, zq], w_ss.at[o - 2], w_rs.at[o - 2], tp_peers[o - 1])
            )
            w_copies[-1].start()
    sent.extend([*w_own, *w_copies])

    loads[2].wait()

    def g_loop(i, carry):
        g_load(i).wait()
        r = dot_nn(gv[pl.ds(pl.multiple_of(i * XR, XR), XR), :], wo[...])
        for h in range(XR // T):
            slope[pl.ds((i * (XR // T) + h) * NP, T), :] = r[h * T : (h + 1) * T]
        return carry

    lax.fori_loop(0, XC, g_loop, 0)

    lane = lax.broadcasted_iota(jnp.int32, (S, L), 1)
    zero = jnp.zeros((S, L), F32)

    def near(ref, t):
        return ref[pl.ds(t, S, stride=NP), :]

    def wide(ref, t):
        return ref[pl.ds(t, S, stride=HP), :]

    def spread(stat, t):
        return jnp.sum(jnp.where(lane == t, stat, 0.0), axis=1, keepdims=True)

    def tap(k):
        return taps[pl.ds(k, 1), :]

    def conv_block(b, carry):
        s1, s2 = carry
        t0 = b * J
        r = [zero] * J
        for i in range(J + H):
            m = wide(hist, t0 + (PAD - H) + i)
            for j in range(J):
                k = H + j - i
                if 0 <= k < K:
                    r[j] = r[j] + tap(k) * m
        for j in range(J):
            convp[t0 + j] = r[j]
            s1 = jnp.where(lane == t0 + j, jnp.sum(r[j], axis=1, keepdims=True), s1)
            s2 = jnp.where(lane == t0 + j, jnp.sum(r[j] * r[j], axis=1, keepdims=True), s2)
        return s1, s2

    def exchange(own, got, ss, rs):
        copies = [remote(own, got.at[i], ss.at[i], rs.at[i], tp_peers[i]) for i in range(7)]
        for cp in copies:
            cp.start()
        sent.extend(copies)
        return copies

    def total(own, got, i):
        r = own[i]
        for p in range(7):
            r = r + got[p, i]
        return r * (1.0 / C)

    near_end = -(-H // J)
    s1, s2 = lax.fori_loop(near_end, T // J, conv_block, (zero, zero))
    halo_m.wait_recv()
    hist[pl.ds(0, PAD), :] = jnp.where(first, 0.0, halo_in[...])
    s1, s2 = lax.fori_loop(0, near_end, conv_block, (s1, s2))
    sta[0] = s1
    sta[1] = s2
    ex = exchange(sta, star, sa_ss, sa_rs)

    for cp in w_copies:
        cp.wait_recv()
    at = wg.at[pl.ds(1, 6), yq, zq]
    w_y = remote(at, at, wy_ss.at[0], wy_rs.at[0], to(y=y + 1 - 2 * yq))
    w_y.start()
    sent.append(w_y)

    for cp in ex:
        cp.wait_recv()
    center = total(sta, star, 0)
    inverse = lax.rsqrt(total(sta, star, 1) - center * center + norm_floor)
    gains = gain[...]

    def norm_block(b, carry):
        gsum, s1, s2 = carry
        t0 = b * J
        for j in range(J):
            t = t0 + j
            iv = jnp.broadcast_to(spread(inverse, t), (S, L))
            n = (convp[t] - spread(center, t)) * iv
            sc = n * gains
            sq = jax.nn.sigmoid(sc)
            act[pl.ds(t, S, stride=NP), :] = sc * sq
            ps = near(slope, t) * sq * (1.0 + sc * (1.0 - sq))
            gsum = gsum + ps * n
            ns = ps * gains
            inv[t] = iv
            nrm[t] = n
            nsl[t] = ns
            s1 = jnp.where(lane == t, jnp.sum(ns, axis=1, keepdims=True), s1)
            s2 = jnp.where(lane == t, jnp.sum(ns * n, axis=1, keepdims=True), s2)
        return gsum, s1, s2

    gsum, s1, s2 = lax.fori_loop(0, T // J, norm_block, (zero, zero, zero))
    stb[0] = s1
    stb[1] = s2
    ex = exchange(stb, stbr, sb_ss, sb_rs)

    at = wg.at[pl.ds(1, 6), 1 - yq, zq]
    remote(at, at, wy_ss.at[0], wy_rs.at[0], to(y=y + 1 - 2 * yq)).wait_recv()
    at = wg.at[pl.ds(1, 6), :, zq]
    w_z = remote(at, at, wy_ss.at[1], wy_rs.at[1], to(z=z + 1 - 2 * zq))
    w_z.start()
    sent.append(w_z)

    def flip(src, dst, row0):
        def step(n, carry):
            dst[pl.ds(row0, L), pl.ds(pl.multiple_of(n * T, T), T)] = src[pl.ds(n * NP, T), :].T.astype(BF16)
            return carry

        lax.fori_loop(0, S, step, 0)

    flip(act, actT, 0)

    def weight_block(left, right, zi, dsts):
        at = pl.ds(pl.multiple_of(zi * (D // Z), D // Z), D // Z)
        r = dot_nn(left[...], right[:, at]).T.astype(BF16)
        for n, dst in enumerate(dsts):
            for yi in range(Y):
                dst[zi, yi] = r[yi * RB : (yi + 1) * RB, n * L : (n + 1) * L]

    def y_send(src, dst, ss, rs):
        copies = []
        for d in range(1, Y):
            copies.append(
                remote(src.at[:, (y + d) % Y], dst.at[d - 1], ss.at[d - 1], rs.at[d - 1], y_peers[d - 1])
            )
            copies[-1].start()
        sent.extend(copies)
        return copies

    def out_loop(zi, carry):
        weight_block(actT, gv, zi, (wgo,))
        return carry

    lax.fori_loop(0, Z, out_loop, 0)

    for cp in ex:
        cp.wait_recv()
    slope_sum = total(stb, stbr, 0)
    cross_sum = total(stb, stbr, 1)

    def cs_block(b, carry):
        t0 = b * J
        for j in range(J):
            t = t0 + j
            cs[pl.ds(t, S, stride=HP), :] = inv[t] * (
                nsl[t] - spread(slope_sum, t) - nrm[t] * spread(cross_sum, t)
            )
        return carry

    lax.fori_loop(0, PAD // J, cs_block, 0)
    halo_out[...] = cs[pl.ds(0, PAD), :]
    halo_c = remote(halo_out, halo_back, h_ss.at[1], h_rs.at[1], prv)
    halo_c.start()
    yo = y_send(wgo, yro, yo_ss, yo_rs)
    for n in range(S - 1):
        cs[pl.ds(n * HP + T, PAD), :] = cs[pl.ds((n + 1) * HP, PAD), :]
    lax.fori_loop(PAD // J, T // J, cs_block, 0)

    def slope_block(b, carry):
        t0 = b * J
        r = [zero] * J
        for i in range(J + H):
            f = wide(cs, t0 + i)
            for j in range(J):
                k = i - j
                if 0 <= k < K:
                    r[j] = r[j] + tap(k) * f
        for j in range(J):
            t = t0 + j
            s = near(sbuf, t)
            rs = r[j] * s
            vsf[pl.ds(t, S, stride=NP), :] = rs
            gsf[pl.ds(t, S, stride=NP), :] = rs * near(vbuf, t) * (1.0 - s)
        return carry

    free = (T - H) // J
    lax.fori_loop(0, free, slope_block, 0)

    def tap_block(b, sums):
        sums = list(sums)
        t0 = b * 8
        e = [wide(cs, t0 + j) for j in range(8)]
        for i in range(8 + H):
            m = wide(hist, t0 + (PAD - H) + i)
            for j in range(8):
                k = H + j - i
                if 0 <= k < K:
                    sums[k] = sums[k] + e[j] * m
        return tuple(sums)

    sums = lax.fori_loop(0, T // 8, tap_block, tuple(zero for _ in range(K)))
    for k in range(K):
        tgs[pl.ds(k, 1), :] = jnp.sum(sums[k], axis=0, keepdims=True)
    tgs[pl.ds(K, 1), :] = jnp.sum(gsum, axis=0, keepdims=True)
    ty = []
    for d in range(1, Y):
        ty.append(remote(tgs, tgy.at[y], ty_ss.at[d - 1], ty_rs.at[d - 1], y_peers[d - 1]))
        ty[-1].start()
    sent.extend(ty)
    tgy[y] = tgs[...]

    halo_c.wait_recv()
    cs[pl.ds((S - 1) * HP + T, PAD), :] = jnp.where(last, 0.0, halo_back[...])
    lax.fori_loop(free, T // J, slope_block, 0)

    def to_bf16(n, carry):
        at = pl.ds(pl.multiple_of(n * T, T), T)
        sl[at, pl.ds(0, L)] = vsf[pl.ds(n * NP, T), :].astype(BF16)
        sl[at, pl.ds(L, L)] = gsf[pl.ds(n * NP, T), :].astype(BF16)
        return carry

    lax.fori_loop(0, S, to_bf16, 0)

    def piece(ref, q):
        return ref.at[pl.ds(q * CH, CH)]

    def own_copy(way, slot, q, dev):
        return remote(piece(sl, q), piece(slg.at[slot], q), own_ss.at[way, q], slg_rs.at[slot, q], dev)

    right, left = to(x=xp), to(x=xm)
    partner = to(c=1 - c)
    up = [own_copy(0, 1, q, right) for q in range(NC)]
    down = [own_copy(1, 2, q, left) for q in range(NC)]
    over = [own_copy(2, 0, q, partner) for q in range(NC)]
    half = NC // 2
    for i in range(NC):
        up[i].start()
        down[(i + half) % NC].start()
    for i in range(NC):
        over[i].start()
    sent.extend([*up, *down, *over])

    flip(vsf, slT, 0)
    flip(gsf, slT, L)

    def gate_send(d):
        return remote(
            wgg.at[(z + 1 + d) % Z], zrg.at[d], zg_ss.at[d], zg_rs.at[d], to(z=(z + 1 + d) % Z)
        )

    def vg_loop(d, carry):
        weight_block(slT, xv, (z + 1 + d) % Z, (wgv, wgg))
        gate_send(d).start()
        return carry

    lax.fori_loop(0, Z - 1, vg_loop, 0)
    weight_block(slT, xv, z, (wgv, wgg))
    yv = y_send(wgv, yrv, yv_ss, yv_rs)
    zg = [gate_send(d) for d in range(Z - 1)]
    sent.extend(zg)

    for cp in w_own:
        cp.wait_recv()
    at = wg.at[pl.ds(1, 6), :, 1 - zq]
    remote(at, at, wy_ss.at[1], wy_rs.at[1], to(z=z + 1 - 2 * zq)).wait_recv()

    def weights_from(slot):
        core = 1 if slot == 0 or slot > 3 else 0
        base = slot if slot <= 3 else slot - 3
        if base == 0:
            return wg[0].reshape(DB, 2 * L)
        if base == 3:
            return wg[3 + core].reshape(DB, 2 * L)
        way = 3 - 2 * (x % 2) if base == 1 else 1 + 2 * (x % 2)
        return wg[2 * way + core - 1].reshape(DB, 2 * L)

    at = pl.ds(pl.multiple_of((x * 2 + c) * DB, DB), DB)
    acc[...] = dot_nt(sl[...], wvg[at, :])

    def add(slot, q):
        at = pl.ds(q * CH, CH)
        acc[at, :] += dot_nt(slg[slot, at, :], weights_from(slot))

    def pf(slot, q):
        cp = remote(
            piece(slg.at[slot], q), piece(slg.at[slot + 3], q), pf_ss.at[slot - 1, q], slg_rs.at[slot + 3, q], partner
        )
        cp.start()
        sent.append(cp)
        return cp

    fwd = {}
    pfs = {}
    for i in range(NC):
        q = i
        up[q].wait_recv()
        if i < half:
            fwd[q] = remote(piece(slg.at[1], q), piece(slg.at[3], q), fwd_ss.at[q], slg_rs.at[3, q], right)
            fwd[q].start()
        pfs[1, q] = pf(1, q)
        q2 = (i + half) % NC
        down[q2].wait_recv()
        if i < half:
            fwd[q2] = remote(piece(slg.at[2], q2), piece(slg.at[3], q2), fwd_ss.at[q2], slg_rs.at[3, q2], left)
            fwd[q2].start()
        pfs[2, q2] = pf(2, q2)
        over[i].wait_recv()
        add(0, i)
        add(1, q)
        add(2, q2)
        if i == half:
            for cp in yo:
                cp.wait_recv()
            zo = second(Z, Y, y, z, wgo, yro, zso, zro, zo_ss, zo_rs, z_peers, remote, sent)
            for cp in ty:
                cp.wait_recv()
            t = tgy[0]
            for yi in range(1, Y):
                t = t + tgy[yi]
            tgzs[...] = t
            tgz[z] = t
            tz = []
            for d in range(1, Z):
                tz.append(remote(tgzs, tgz.at[z], tz_ss.at[d - 1], tz_rs.at[d - 1], z_peers[d - 1]))
                tz[-1].start()
            sent.extend(tz)
    sent.extend(fwd.values())
    for q in range(NC):
        pfs[1, q].wait_recv()
        add(4, q)
        pfs[2, q].wait_recv()
        add(5, q)

    for cp in yv:
        cp.wait_recv()
    zv = second(Z, Y, y, z, wgv, yrv, zsv, zrv, zv_ss, zv_rs, z_peers, remote, sent)
    for cp in zg:
        cp.wait_recv()
    for yi in range(Y):
        r = wgg[z, yi].astype(F32)
        for d in range(Z - 1):
            r = r + zrg[d, yi].astype(F32)
        ysg[yi] = r.astype(BF16)
    yg = []
    for d in range(1, Y):
        yg.append(remote(ysg.at[(y + d) % Y], yrg.at[d - 1], yg_ss.at[d - 1], yg_rs.at[d - 1], y_peers[d - 1]))
        yg[-1].start()
    sent.extend(yg)

    order = [q for i in range(half) for q in (i, i + half)]
    for q in order:
        fwd[q].wait_recv()
        pfs[3, q] = pf(3, q)
        add(3, q)
    for q in order:
        pfs[3, q].wait_recv()
        add(6, q)
    ig[...] = acc[...].astype(BF16)

    def finish(copies, own, got, count):
        for cp in copies:
            cp.wait_recv()
        r = own.astype(F32)
        for d in range(count - 1):
            r = r + got[d].astype(F32)
        return r

    og[...] = finish(zo, zso[z], zro, Z)
    for cp in tz:
        cp.wait_recv()
    t = tgz[0]
    for zi in range(1, Z):
        t = t + tgz[zi]
    tg[...] = t[:K]
    ng[...] = t[K : K + 1]
    vg[...] = finish(zv, zsv[z], zrv, Z)
    gg[...] = finish(yg, ysg[y], yrg, Y)

    for cp in [halo_m, halo_c, *sent]:
        cp.wait_send()


def second(Z, Y, y, z, own, got, zs, zr, ss, rs, z_peers, remote, sent):
    def step(zi, carry):
        r = own[zi, y].astype(F32)
        for d in range(Y - 1):
            r = r + got[d, zi].astype(F32)
        zs[zi] = r.astype(BF16)
        return carry

    lax.fori_loop(0, Z, step, 0)
    copies = []
    for d in range(1, Z):
        copies.append(remote(zs.at[(z + d) % Z], zr.at[d - 1], ss.at[d - 1], rs.at[d - 1], z_peers[d - 1]))
        copies[-1].start()
    sent.extend(copies)
    return copies


def write_out(*refs):
    half = len(refs) // 2
    for src, dst in zip(refs[:half], refs[half:]):
        dst[...] = src[...]


def shards(Z, Y, block_input, value_proj, gate_proj, conv_taps, norm_gain, out_proj, grad_output):
    rows, D = block_input.shape
    K = conv_taps.shape[0]
    C = value_proj.shape[1] * 8
    DB, RB, T = D // 8, D // (Z * Y), rows // S
    vm = pltpu.VMEM
    dma = pltpu.SemaphoreType.DMA
    hbm, vmem = pl.BlockSpec(memory_space=ANYWHERE), pl.BlockSpec(memory_space=pltpu.VMEM)
    near, wide = vm((S * NP, L), F32), vm((S * HP, L), F32)
    flat = vm((T, S, L), F32)
    halo = vm((PAD, L), F32)
    stat, stats = vm((2, S, L), F32), vm((7, 2, S, L), F32)
    scratch = [
        vm((rows, D), BF16), vm((rows, D), BF16), vm((D, 2 * L), BF16), vm((D, L), BF16), vm((7, 2, 2, DB // 4, 2 * L), BF16),
        near, near, near, wide, flat, flat, flat, flat, near, wide,
        near, near, vm((rows, 2 * L), BF16), vm((7, rows, 2 * L), BF16), vm((rows, DB), F32),
        halo, halo, halo, halo,
        vm((L, rows), BF16), vm((2 * L, rows), BF16),
        *[vm((Z, Y, RB, L), BF16) for _ in range(3)],
        vm((Y - 1, Z, RB, L), BF16), vm((Y - 1, Z, RB, L), BF16),
        vm((Z, RB, L), BF16), vm((Z, RB, L), BF16), vm((Z - 1, RB, L), BF16), vm((Z - 1, RB, L), BF16),
        vm((Z - 1, Y, RB, L), BF16), vm((Y, RB, L), BF16), vm((Y - 1, RB, L), BF16),
        stat, stats, stat, stats,
        halo, vm((Y, PAD, L), F32), halo, vm((Z, PAD, L), F32),
        dma((3,)), dma((4,)), dma((4,)), dma((4,)), dma((4,)), dma((6,)), dma((6,)), dma((2,)), dma((2,)), dma((2,)), dma((2,)),
        dma((7,)), dma((7,)), dma((7,)), dma((7,)), dma((3, NC)), dma((NC,)), dma((3, NC)), dma((7, NC)),
        *[dma((Y - 1,)) for _ in range(6)], *[dma((Z - 1,)) for _ in range(6)],
        dma((Y - 1,)), dma((Y - 1,)), dma((Z - 1,)), dma((Z - 1,)),
    ]
    shapes = (
        jax.ShapeDtypeStruct((rows, DB), BF16),
        jax.ShapeDtypeStruct((RB, L), F32),
        jax.ShapeDtypeStruct((RB, L), F32),
        jax.ShapeDtypeStruct((RB, L), F32),
        jax.ShapeDtypeStruct((K, L), F32),
        jax.ShapeDtypeStruct((1, L), F32),
    )
    block_input, value_proj, gate_proj, out_proj, grad_output = (
        pltpu.with_memory_space_constraint(a, pltpu.HBM)
        for a in (block_input, value_proj, gate_proj, out_proj, grad_output)
    )
    outs = pl.pallas_call(
        functools.partial(body, Z, Y, C, K),
        out_shape=shapes,
        in_specs=[hbm, hbm, hbm, vmem, vmem, hbm, hbm],
        out_specs=[vmem] * 6,
        scratch_shapes=scratch,
        compiler_params=pltpu.CompilerParams(
            collective_id=0, has_side_effects=True, vmem_limit_bytes=VMEM_LIMIT
        ),
        name="block_backward",
    )(block_input, value_proj, gate_proj, conv_taps, norm_gain.reshape(1, L), out_proj, grad_output)
    outs = pl.pallas_call(
        write_out,
        out_shape=shapes,
        in_specs=[vmem] * 6,
        out_specs=[vmem] * 6,
        compiler_params=pltpu.CompilerParams(vmem_limit_bytes=4 * 1024 * 1024),
        name="write_out",
    )(*outs)
    return (*outs[:5], outs[5].reshape(L))


def solution(mesh):
    tp = mesh.shape["tp"]
    Y = 4
    Z = mesh.shape["sp"] // Y
    finer = Mesh(mesh.devices.reshape(Z, Y, tp // 2, 2), ("z", "y", "x", "c"))
    sp, ch = ("z", "y"), ("x", "c")
    return jax.shard_map(
        functools.partial(shards, Z, Y),
        mesh=finer,
        in_specs=(P(sp, None), P(None, ch), P(None, ch), P(None, ch), P(ch), P(None, ch), P(sp, None)),
        out_specs=(P(sp, ch), P(sp, ch), P(sp, ch), P(sp, ch), P(None, ch), P(ch)),
        check_vma=False,
    )
```

```python
import functools

import jax
import jax.numpy as jnp
from jax import lax
from jax.experimental import pallas as pl
from jax.experimental.pallas import tpu as pltpu
from jax.sharding import Mesh
from jax.sharding import PartitionSpec as P

MESH = pl.DeviceIdType.MESH
F32 = jnp.float32
BF16 = jnp.bfloat16
norm_floor = 0.1
ANYWHERE = pltpu.HBM
VMEM_LIMIT = 40 * 1024 * 1024
L = 128
S = 8
J = 16
NP = 132
HP = 164
PAD = 32
NN = 4
FAR0, NF = 3, 3
NC = 4


def dot_nn(a, b):
    return lax.dot_general(a, b, (((1,), (0,)), ((), ())), preferred_element_type=F32)


def dot_nt(a, b):
    return lax.dot_general(a, b, (((1,), (1,)), ((), ())), preferred_element_type=F32)


def body(
    Z, Y, C, K,
    x_hbm, vp_hbm, gp_hbm, taps_hbm, gain_hbm, op_hbm, g_hbm,
    ig, vg, gg, og, tg, ng,
    xv, gv, wvg, wo, wg, vbuf, sbuf, slope, hist, convp, nrm, nsl, inv, act, cs, vsf, gsf, sl, slg, acc,
    tail, halo_in, halo_out, halo_back, taps, gain,
    actT, slT, wgo, wvf, wvn, wgn, yro, yrf, yrv, zso, zsf, zsv, zro, zrf, zrv, zrg, ysg, yrg, sta, star, stb, stbr, tgs, tgy, tgzs, tgz,
    in_sem, l_sem, x_sem, g_sem, wo_ss, wo_rs, w_ss, w_rs, wy_ss, wy_rs, h_ss, h_rs, sa_ss, sa_rs, sb_ss, sb_rs, own_ss, fwd_ss, pf_ss, slg_rs,
    yo_ss, yo_rs, yf_ss, yf_rs, yv_ss, yv_rs, yg_ss, yg_rs, zo_ss, zo_rs, zf_ss, zf_rs, zv_ss, zv_rs, zg_ss, zg_rs,
    ty_ss, ty_rs, tz_ss, tz_rs,
):
    z, y, x, c = (lax.axis_index(a) for a in ("z", "y", "x", "c"))
    rows, D = xv.shape
    T = rows // S
    DB = D // 8
    DQ = DB // 4
    RB = D // (Z * Y)
    CH = rows // NC
    H = K - 1

    yn = (y + 1) % Y
    zn = (z + (y + 1) // Y) % Z
    yb = (y + Y - 1) % Y
    zb = (z + Z - 1 + (y + Y - 1) // Y) % Z
    first = (z + y) == 0
    last = (z * Y + y) == (Z * Y - 1)
    xp, xm = (x + 1) % 4, (x + 3) % 4
    xs = (x, x + 1 - 2 * (x % 2), (x + 2) % 4, 3 - x)
    cc = (c, 1 - c)

    def to(z=z, y=y, x=x, c=c):
        return {"z": z, "y": y, "x": x, "c": c}

    def remote(src, dst, ss, rs, dev):
        return pltpu.make_async_remote_copy(
            src_ref=src, dst_ref=dst, send_sem=ss, recv_sem=rs, device_id=dev, device_id_type=MESH
        )

    tp_peers = [to(x=xs[o // 2], c=cc[o % 2]) for o in range(1, 8)]
    y_peers = [to(y=(y + d) % Y) for d in range(1, Y)]
    z_peers = [to(z=(z + d) % Z) for d in range(1, Z)]
    nxt, prv = to(z=zn, y=yn), to(z=zb, y=yb)
    sent = []

    loads = [
        pltpu.make_async_copy(vp_hbm, wvg.at[:, pl.ds(0, L)], l_sem.at[0]),
        pltpu.make_async_copy(gp_hbm, wvg.at[:, pl.ds(L, L)], l_sem.at[1]),
        pltpu.make_async_copy(op_hbm, wo, l_sem.at[2]),
        pltpu.make_async_copy(taps_hbm, taps, l_sem.at[3]),
        pltpu.make_async_copy(gain_hbm, gain, l_sem.at[4]),
    ]
    loads[0].start()
    loads[1].start()
    XC = 4
    XR = rows // XC

    def x_load(i):
        at = pl.ds(pl.multiple_of(i * XR, XR), XR)
        return pltpu.make_async_copy(x_hbm.at[at], xv.at[at], x_sem.at[i])

    def g_load(i):
        at = pl.ds(pl.multiple_of(i * XR, XR), XR)
        return pltpu.make_async_copy(g_hbm.at[at], gv.at[at], g_sem.at[i])

    for i in (XC - 1, *range(XC - 1)):
        x_load(i).start()
    for cp in loads[2:]:
        cp.start()
    for i in range(XC):
        g_load(i).start()

    barrier = pltpu.get_barrier_semaphore()
    for dev in (*tp_peers, *y_peers):
        pl.semaphore_signal(barrier, inc=1, device_id=dev, device_id_type=MESH)
    below, above = z > 0, z < Z - 1
    into, out_of = (y == 0) & below, (y == Y - 1) & above
    for there, dev in (
        (below, to(z=(z + Z - 1) % Z)),
        (above, to(z=(z + 1) % Z)),
        (into, prv),
        (out_of, nxt),
    ):

        @pl.when(there)
        def _(dev=dev):
            pl.semaphore_signal(barrier, inc=1, device_id=dev, device_id_type=MESH)

    greeted = len(tp_peers) + len(y_peers) + sum(
        jnp.where(there, 1, 0) for there in (below, above, into, out_of)
    )

    def pass_on(k):
        n = 2**k
        for i, there, at in ((0, z + n < Z, (z + n) % Z), (1, z >= n, (z + Z - n) % Z)):

            @pl.when(there)
            def _(i=i, at=at):
                pl.semaphore_signal(in_sem.at[2 * k + i], inc=1, device_id=to(z=at), device_id_type=MESH)

    def heard(k):
        n = 2**k
        for i, there in ((0, z >= n), (1, z + n < Z)):

            @pl.when(there)
            def _(i=i):
                pl.semaphore_wait(in_sem.at[2 * k + i], 1)


    loads[0].wait()
    loads[1].wait()

    def x_step(i, end):
        x_load(i).wait()
        res = dot_nn(xv[pl.ds(pl.multiple_of(i * XR, XR), XR), :], wvg[...])
        v = res[:, :L]
        s = jax.nn.sigmoid(res[:, L:])
        m = (v * s).astype(BF16).astype(F32)
        for h in range(XR // T):
            n = i * (XR // T) + h
            part = slice(h * T, (h + 1) * T)
            vbuf[pl.ds(n * NP, T), :] = v[part]
            sbuf[pl.ds(n * NP, T), :] = s[part]
            hist[pl.ds(n * HP + PAD, T), :] = m[part]
            if end and h == XR // T - 1:
                tail[...] = m[XR - PAD :]
            else:
                hist[pl.ds((n + 1) * HP, PAD), :] = m[(h + 1) * T - PAD : (h + 1) * T]

    x_step(XC - 1, True)

    def x_loop(i, carry):
        x_step(i, False)
        return carry

    x_step(0, False)

    pl.semaphore_wait(barrier, greeted)
    halo_m = remote(tail, halo_in, h_ss.at[0], h_rs.at[0], nxt)

    @pl.when(jnp.logical_not(last))
    def _():
        halo_m.start()

    pass_on(0)

    yq, zq = y % 2, z % 2
    w_copies, w_own = [], []
    for o in range(1, 8):
        px, pc = xs[o // 2], cc[o % 2]
        row = (px * 2 + pc) * DB
        if o == 1:
            for i in range(4):
                at = pl.ds(pl.multiple_of(row + i * DQ, DQ), DQ)
                w_own.append(remote(wvg.at[at], wg.at[0, i // 2, i % 2], wo_ss.at[i], wo_rs.at[i], tp_peers[0]))
                w_own[-1].start()
        else:
            at = pl.ds(pl.multiple_of(row + (2 * yq + zq) * DQ, DQ), DQ)
            w_copies.append(
                remote(wvg.at[at], wg.at[o - 1, yq, zq], w_ss.at[o - 2], w_rs.at[o - 2], tp_peers[o - 1])
            )
            w_copies[-1].start()
    sent.extend([*w_own, *w_copies])

    lax.fori_loop(1, XC - 1, x_loop, 0)

    for cp in loads[2:]:
        cp.wait()

    def g_loop(i, carry):
        g_load(i).wait()
        r = dot_nn(gv[pl.ds(pl.multiple_of(i * XR, XR), XR), :], wo[...])
        for h in range(XR // T):
            slope[pl.ds((i * (XR // T) + h) * NP, T), :] = r[h * T : (h + 1) * T]
        return carry

    lax.fori_loop(0, XC, g_loop, 0)

    lane = lax.broadcasted_iota(jnp.int32, (S, L), 1)
    zero = jnp.zeros((S, L), F32)

    def near(ref, t):
        return ref[pl.ds(t, S, stride=NP), :]

    def wide(ref, t):
        return ref[pl.ds(t, S, stride=HP), :]

    def spread(stat, t):
        return jnp.sum(jnp.where(lane == t, stat, 0.0), axis=1, keepdims=True)

    def tap(k):
        return taps[pl.ds(k, 1), :]

    def conv_block(b, carry):
        s1, s2 = carry
        t0 = b * J
        r = [zero] * J
        for i in range(J + H):
            m = wide(hist, t0 + (PAD - H) + i)
            for j in range(J):
                k = H + j - i
                if 0 <= k < K:
                    r[j] = r[j] + tap(k) * m
        for j in range(J):
            convp[t0 + j] = r[j]
            s1 = jnp.where(lane == t0 + j, jnp.sum(r[j], axis=1, keepdims=True), s1)
            s2 = jnp.where(lane == t0 + j, jnp.sum(r[j] * r[j], axis=1, keepdims=True), s2)
        return s1, s2

    def exchange(own, got, ss, rs):
        copies = [remote(own, got.at[i], ss.at[i], rs.at[i], tp_peers[i]) for i in range(7)]
        for cp in copies:
            cp.start()
        sent.extend(copies)
        return copies

    def total(own, got, i):
        r = own[i]
        for p in range(7):
            r = r + got[p, i]
        return r * (1.0 / C)

    near_end = -(-H // J)
    s1, s2 = lax.fori_loop(near_end, T // J, conv_block, (zero, zero))

    @pl.when(first)
    def _():
        hist[pl.ds(0, PAD), :] = jnp.zeros((PAD, L), F32)

    @pl.when(jnp.logical_not(first))
    def _():
        halo_m.wait_recv()
        hist[pl.ds(0, PAD), :] = halo_in[...]

    s1, s2 = lax.fori_loop(0, near_end, conv_block, (s1, s2))
    sta[0] = s1
    sta[1] = s2
    ex = exchange(sta, star, sa_ss, sa_rs)

    for cp in w_copies:
        cp.wait_recv()
    at = wg.at[pl.ds(1, 6), yq, zq]
    w_on = [
        remote(at, at, wy_ss.at[0], wy_rs.at[0], to(y=y + 1 - 2 * yq)),
        remote(at, at, wy_ss.at[1], wy_rs.at[1], to(z=z + 1 - 2 * zq)),
    ]
    for cp in w_on:
        cp.start()
    sent.extend(w_on)
    heard(0)
    pass_on(1)

    for cp in ex:
        cp.wait_recv()
    center = total(sta, star, 0)
    inverse = lax.rsqrt(total(sta, star, 1) - center * center + norm_floor)
    gains = gain[...]

    def norm_block(b, carry):
        gsum, s1, s2 = carry
        t0 = b * J
        for j in range(J):
            t = t0 + j
            iv = jnp.broadcast_to(spread(inverse, t), (S, L))
            n = (convp[t] - spread(center, t)) * iv
            sc = n * gains
            sq = jax.nn.sigmoid(sc)
            act[pl.ds(t, S, stride=NP), :] = sc * sq
            ps = near(slope, t) * sq * (1.0 + sc * (1.0 - sq))
            gsum = gsum + ps * n
            ns = ps * gains
            inv[t] = iv
            nrm[t] = n
            nsl[t] = ns
            s1 = jnp.where(lane == t, jnp.sum(ns, axis=1, keepdims=True), s1)
            s2 = jnp.where(lane == t, jnp.sum(ns * n, axis=1, keepdims=True), s2)
        return gsum, s1, s2

    gsum, s1, s2 = lax.fori_loop(0, T // J, norm_block, (zero, zero, zero))
    stb[0] = s1
    stb[1] = s2
    ex = exchange(stb, stbr, sb_ss, sb_rs)
    heard(1)
    pass_on(2)

    def flip(src, dst, row0):
        def step(n, carry):
            dst[pl.ds(row0, L), pl.ds(pl.multiple_of(n * T, T), T)] = src[pl.ds(n * NP, T), :].T.astype(BF16)
            return carry

        lax.fori_loop(0, S, step, 0)

    flip(act, actT, 0)

    def weight_block(left, right, zi, put):
        at = pl.ds(pl.multiple_of(zi * (D // Z), D // Z), D // Z)
        r = dot_nn(left[...], right[:, at]).T.astype(BF16)
        for yi in range(Y):
            put(yi, r[yi * RB : (yi + 1) * RB])

    def y_send(src, dst, ss, rs):
        copies = []
        for d in range(1, Y):
            copies.append(
                remote(src.at[:, (y + d) % Y], dst.at[d - 1], ss.at[d - 1], rs.at[d - 1], y_peers[d - 1])
            )
            copies[-1].start()
        sent.extend(copies)
        return copies

    def out_loop(zi, carry):
        def put(yi, r):
            wgo[zi, yi] = r

        weight_block(actT, gv, zi, put)
        return carry

    lax.fori_loop(0, Z, out_loop, 0)

    for cp in ex:
        cp.wait_recv()
    slope_sum = total(stb, stbr, 0)
    cross_sum = total(stb, stbr, 1)

    def cs_block(b, carry):
        t0 = b * J
        for j in range(J):
            t = t0 + j
            cs[pl.ds(t, S, stride=HP), :] = inv[t] * (
                nsl[t] - spread(slope_sum, t) - nrm[t] * spread(cross_sum, t)
            )
        return carry

    lax.fori_loop(0, PAD // J, cs_block, 0)
    halo_out[...] = cs[pl.ds(0, PAD), :]
    halo_c = remote(halo_out, halo_back, h_ss.at[1], h_rs.at[1], prv)

    @pl.when(jnp.logical_not(first))
    def _():
        halo_c.start()

    at = wg.at[pl.ds(1, 6), 1 - yq, zq]
    remote(at, at, wy_ss.at[0], wy_rs.at[0], to(y=y + 1 - 2 * yq)).wait_recv()
    w_z = remote(at, at, wy_ss.at[2], wy_rs.at[2], to(z=z + 1 - 2 * zq))
    w_z.start()
    sent.append(w_z)
    yo = y_send(wgo, yro, yo_ss, yo_rs)
    for n in range(S - 1):
        cs[pl.ds(n * HP + T, PAD), :] = cs[pl.ds((n + 1) * HP, PAD), :]
    lax.fori_loop(PAD // J, T // J, cs_block, 0)

    def slope_block(b, carry):
        t0 = b * J
        r = [zero] * J
        for i in range(J + H):
            f = wide(cs, t0 + i)
            for j in range(J):
                k = i - j
                if 0 <= k < K:
                    r[j] = r[j] + tap(k) * f
        for j in range(J):
            t = t0 + j
            s = near(sbuf, t)
            rs = r[j] * s
            vsf[pl.ds(t, S, stride=NP), :] = rs
            gsf[pl.ds(t, S, stride=NP), :] = rs * near(vbuf, t) * (1.0 - s)
        return carry

    free = (T - H) // J
    lax.fori_loop(0, free, slope_block, 0)

    def tap_block(b, sums):
        sums = list(sums)
        t0 = b * 8
        e = [wide(cs, t0 + j) for j in range(8)]
        for i in range(8 + H):
            m = wide(hist, t0 + (PAD - H) + i)
            for j in range(8):
                k = H + j - i
                if 0 <= k < K:
                    sums[k] = sums[k] + e[j] * m
        return tuple(sums)

    sums = lax.fori_loop(0, T // 8, tap_block, tuple(zero for _ in range(K)))
    for k in range(K):
        tgs[pl.ds(k, 1), :] = jnp.sum(sums[k], axis=0, keepdims=True)
    tgs[pl.ds(K, 1), :] = jnp.sum(gsum, axis=0, keepdims=True)
    ty = []
    for d in range(1, Y):
        ty.append(remote(tgs, tgy.at[y], ty_ss.at[d - 1], ty_rs.at[d - 1], y_peers[d - 1]))
        ty[-1].start()
    sent.extend(ty)
    tgy[y] = tgs[...]


    @pl.when(last)
    def _():
        cs[pl.ds((S - 1) * HP + T, PAD), :] = jnp.zeros((PAD, L), F32)

    @pl.when(jnp.logical_not(last))
    def _():
        halo_c.wait_recv()
        cs[pl.ds((S - 1) * HP + T, PAD), :] = halo_back[...]

    lax.fori_loop(free, T // J, slope_block, 0)

    def to_bf16(n, carry):
        at = pl.ds(pl.multiple_of(n * T, T), T)
        sl[at, pl.ds(0, L)] = vsf[pl.ds(n * NP, T), :].astype(BF16)
        sl[at, pl.ds(L, L)] = gsf[pl.ds(n * NP, T), :].astype(BF16)
        return carry

    lax.fori_loop(0, S, to_bf16, 0)

    def piece(ref, q):
        return ref.at[pl.ds(q * CH, CH)]

    def own_copy(way, slot, q, dev):
        return remote(piece(sl, q), piece(slg.at[slot], q), own_ss.at[way, q], slg_rs.at[slot, q], dev)

    right, left = to(x=xp), to(x=xm)
    partner = to(c=1 - c)
    up = [own_copy(0, 1, q, right) for q in range(NC)]
    down = [own_copy(1, 2, q, left) for q in range(NC)]
    over = [own_copy(2, 0, q, partner) for q in range(NC)]
    half = NC // 2
    for i in range(NC):
        up[i].start()
        down[(i + half) % NC].start()
    for i in range(NC):
        over[i].start()
    sent.extend([*up, *down, *over])

    flip(vsf, slT, 0)
    flip(gsf, slT, L)

    def far_loop(e, carry):
        def put(yi, r):
            wvf[e, yi] = r

        weight_block(slT, xv, (z + FAR0 + e) % Z, put)
        return carry

    def near_of(e):
        return (z + Z + (1 + e // 2) * (1 - 2 * (e % 2))) % Z

    def near_from(e):
        return (z + Z - (1 + e // 2) * (1 - 2 * (e % 2))) % Z

    def gate_send(e):
        return remote(wgn.at[e], zrg.at[e], zg_ss.at[e], zg_rs.at[e], to(z=near_of(e)))

    def near_put(e):
        def put(yi, r):
            wvn[e, yi] = r[:, :L]
            wgn[e, yi] = r[:, L:]

        return put

    def near_loop(e, carry):
        weight_block(slT, xv, near_of(e), near_put(e))
        gate_send(e).start()
        return carry

    heard(2)
    lax.fori_loop(0, NF, far_loop, 0)
    yf = y_send(wvf, yrf, yf_ss, yf_rs)
    lax.fori_loop(0, NN, near_loop, 0)
    weight_block(slT, xv, z, near_put(NN))
    yv = y_send(wvn, yrv, yv_ss, yv_rs)
    zg = [gate_send(e) for e in range(NN)]
    sent.extend(zg)

    for cp in yo:
        cp.wait_recv()
    zo = second(Z, Y, y, z, wgo, yro, zso, zro, zo_ss, zo_rs, z_peers, remote, sent)

    def weights_from(slot):
        core = 1 if slot == 0 or slot > 3 else 0
        base = slot if slot <= 3 else slot - 3
        if base == 0:
            return wg[0].reshape(DB, 2 * L)
        if base == 3:
            return wg[3 + core].reshape(DB, 2 * L)
        way = 3 - 2 * (x % 2) if base == 1 else 1 + 2 * (x % 2)
        return wg[2 * way + core - 1].reshape(DB, 2 * L)

    at = pl.ds(pl.multiple_of((x * 2 + c) * DB, DB), DB)
    acc[...] = dot_nt(sl[...], wvg[at, :])

    def add(slot, q):
        at = pl.ds(q * CH, CH)
        acc[at, :] += dot_nt(slg[slot, at, :], weights_from(slot))

    def pf(slot, q):
        cp = remote(
            piece(slg.at[slot], q), piece(slg.at[slot + 3], q), pf_ss.at[slot - 1, q], slg_rs.at[slot + 3, q], partner
        )
        cp.start()
        sent.append(cp)
        return cp

    fwd = {}
    pfs = {}
    for i in range(NC):
        q = i
        up[q].wait_recv()
        if i < half:
            fwd[q] = remote(piece(slg.at[1], q), piece(slg.at[3], q), fwd_ss.at[q], slg_rs.at[3, q], right)
            fwd[q].start()
        pfs[1, q] = pf(1, q)
        q2 = (i + half) % NC
        down[q2].wait_recv()
        if i < half:
            fwd[q2] = remote(piece(slg.at[2], q2), piece(slg.at[3], q2), fwd_ss.at[q2], slg_rs.at[3, q2], left)
            fwd[q2].start()
        pfs[2, q2] = pf(2, q2)
        over[i].wait_recv()
        if i == 1:
            for cp in w_own:
                cp.wait_recv()
            for k, yi in ((1, yq), (2, 1 - yq)):
                at = wg.at[pl.ds(1, 6), yi, 1 - zq]
                remote(at, at, wy_ss.at[k], wy_rs.at[k], to(z=z + 1 - 2 * zq)).wait_recv()
        for j in {0: (), 1: (0, 1)}.get(i, (i,)):
            add(0, j)
            add(1, j)
            add(2, (j + half) % NC)
        if i == 1:
            for cp in ty:
                cp.wait_recv()
            t = tgy[0]
            for yi in range(1, Y):
                t = t + tgy[yi]
            tgzs[...] = t
            tgz[z] = t
            tz = []
            for d in range(1, Z):
                tz.append(remote(tgzs, tgz.at[z], tz_ss.at[d - 1], tz_rs.at[d - 1], z_peers[d - 1]))
                tz[-1].start()
            sent.extend(tz)
        if i == 2:
            for cp in yf:
                cp.wait_recv()
            zf = []
            for e in range(NF):
                r = wvf[e, y].astype(F32)
                for d in range(Y - 1):
                    r = r + yrf[d, e].astype(F32)
                zsf[e] = r.astype(BF16)
                zf.append(remote(zsf.at[e], zrf.at[e], zf_ss.at[e], zf_rs.at[e], to(z=(z + FAR0 + e) % Z)))
                zf[-1].start()
            sent.extend(zf)
            for cp in zg:
                cp.wait_recv()
            for yi in range(Y):
                r = wgn[NN, yi].astype(F32)
                for e in range(NN):
                    r = r + zrg[e, yi].astype(F32)
                ysg[yi] = r.astype(BF16)
            yg = []
            for d in range(1, Y):
                yg.append(
                    remote(ysg.at[(y + d) % Y], yrg.at[d - 1], yg_ss.at[d - 1], yg_rs.at[d - 1], y_peers[d - 1])
                )
                yg[-1].start()
            sent.extend(yg)
        if i == 3:
            for cp in yv:
                cp.wait_recv()
            zv = []
            for e in range(NN + 1):
                r = wvn[e, y].astype(F32)
                for d in range(Y - 1):
                    r = r + yrv[d, e].astype(F32)
                zsv[e] = r.astype(BF16)
                if e < NN:
                    zv.append(remote(zsv.at[e], zrv.at[e], zv_ss.at[e], zv_rs.at[e], to(z=near_of(e))))
                    zv[-1].start()
            sent.extend(zv)
    sent.extend(fwd.values())
    for q in range(NC):
        pfs[1, q].wait_recv()
        add(4, q)
        pfs[2, q].wait_recv()
        add(5, q)

    order = [q for i in range(half) for q in (i, i + half)]
    for q in order:
        fwd[q].wait_recv()
        pfs[3, q] = pf(3, q)
        add(3, q)
    for q in order:
        pfs[3, q].wait_recv()
        add(6, q)
    ig[...] = acc[...].astype(BF16)

    def finish(copies, own, got, count):
        for cp in copies:
            cp.wait_recv()
        r = own.astype(F32)
        for d in range(count - 1):
            r = r + got[d].astype(F32)
        return r

    og[...] = finish(zo, zso[z], zro, Z)
    for cp in tz:
        cp.wait_recv()
    t = tgz[0]
    for zi in range(1, Z):
        t = t + tgz[zi]
    tg[...] = t[:K]
    ng[...] = t[K : K + 1]
    for cp in [*zf, *zv, *yg]:
        cp.wait_recv()
    far = zrf[0].astype(F32)
    for e in range(1, NF):
        far = far + zrf[e].astype(F32)
    r = far[:, :L] + zsv[NN].astype(F32)
    for e in range(NN):
        r = r + zrv[e].astype(F32)
    vg[...] = r
    r = far[:, L:] + ysg[y].astype(F32)
    for d in range(Y - 1):
        r = r + yrg[d].astype(F32)
    gg[...] = r

    for cp in sent:
        cp.wait_send()

    @pl.when(jnp.logical_not(last))
    def _():
        halo_m.wait_send()

    @pl.when(jnp.logical_not(first))
    def _():
        halo_c.wait_send()


def second(Z, Y, y, z, own, got, zs, zr, ss, rs, z_peers, remote, sent):
    def step(zi, carry):
        r = own[zi, y].astype(F32)
        for d in range(Y - 1):
            r = r + got[d, zi].astype(F32)
        zs[zi] = r.astype(BF16)
        return carry

    lax.fori_loop(0, Z, step, 0)
    copies = []
    for d in range(1, Z):
        copies.append(remote(zs.at[(z + d) % Z], zr.at[d - 1], ss.at[d - 1], rs.at[d - 1], z_peers[d - 1]))
        copies[-1].start()
    sent.extend(copies)
    return copies


def write_out(*refs):
    half = len(refs) // 2
    for src, dst in zip(refs[:half], refs[half:]):
        dst[...] = src[...]


def shards(Z, Y, block_input, value_proj, gate_proj, conv_taps, norm_gain, out_proj, grad_output):
    rows, D = block_input.shape
    K = conv_taps.shape[0]
    C = value_proj.shape[1] * 8
    DB, RB, T = D // 8, D // (Z * Y), rows // S
    vm = pltpu.VMEM
    dma = pltpu.SemaphoreType.DMA
    hbm, vmem = pl.BlockSpec(memory_space=ANYWHERE), pl.BlockSpec(memory_space=pltpu.VMEM)
    near, wide = vm((S * NP, L), F32), vm((S * HP, L), F32)
    flat = vm((T, S, L), F32)
    halo = vm((PAD, L), F32)
    stat, stats = vm((2, S, L), F32), vm((7, 2, S, L), F32)
    scratch = [
        vm((rows, D), BF16), vm((rows, D), BF16), vm((D, 2 * L), BF16), vm((D, L), BF16), vm((7, 2, 2, DB // 4, 2 * L), BF16),
        near, near, near, wide, flat, flat, flat, flat, near, wide,
        near, near, vm((rows, 2 * L), BF16), vm((7, rows, 2 * L), BF16), vm((rows, DB), F32),
        halo, halo, halo, halo, vm((K, L), F32), vm((1, L), F32),
        vm((L, rows), BF16), vm((2 * L, rows), BF16),
        vm((Z, Y, RB, L), BF16), vm((NF, Y, RB, 2 * L), BF16), vm((NN + 1, Y, RB, L), BF16), vm((NN + 1, Y, RB, L), BF16),
        vm((Y - 1, Z, RB, L), BF16), vm((Y - 1, NF, RB, 2 * L), BF16), vm((Y - 1, NN + 1, RB, L), BF16),
        vm((Z, RB, L), BF16), vm((NF, RB, 2 * L), BF16), vm((NN + 1, RB, L), BF16),
        vm((Z - 1, RB, L), BF16), vm((NF, RB, 2 * L), BF16), vm((NN, RB, L), BF16),
        vm((NN, Y, RB, L), BF16), vm((Y, RB, L), BF16), vm((Y - 1, RB, L), BF16),
        stat, stats, stat, stats,
        halo, vm((Y, PAD, L), F32), halo, vm((Z, PAD, L), F32),
        pltpu.SemaphoreType.REGULAR((6,)),
        dma((5,)), dma((4,)), dma((4,)), dma((4,)), dma((4,)), dma((6,)), dma((6,)), dma((3,)), dma((3,)), dma((2,)), dma((2,)),
        dma((7,)), dma((7,)), dma((7,)), dma((7,)), dma((3, NC)), dma((NC,)), dma((3, NC)), dma((7, NC)),
        *[dma((Y - 1,)) for _ in range(8)], dma((Z - 1,)), dma((Z - 1,)), dma((NF,)), dma((NF,)), *[dma((NN,)) for _ in range(4)],
        dma((Y - 1,)), dma((Y - 1,)), dma((Z - 1,)), dma((Z - 1,)),
    ]
    shapes = (
        jax.ShapeDtypeStruct((rows, DB), BF16),
        jax.ShapeDtypeStruct((RB, L), F32),
        jax.ShapeDtypeStruct((RB, L), F32),
        jax.ShapeDtypeStruct((RB, L), F32),
        jax.ShapeDtypeStruct((K, L), F32),
        jax.ShapeDtypeStruct((1, L), F32),
    )
    norm_gain = norm_gain.reshape(1, L)
    block_input, value_proj, gate_proj, conv_taps, norm_gain, out_proj, grad_output = (
        pltpu.with_memory_space_constraint(a, pltpu.HBM)
        for a in (block_input, value_proj, gate_proj, conv_taps, norm_gain, out_proj, grad_output)
    )
    outs = pl.pallas_call(
        functools.partial(body, Z, Y, C, K),
        out_shape=shapes,
        in_specs=[hbm] * 7,
        out_specs=[vmem] * 6,
        scratch_shapes=scratch,
        compiler_params=pltpu.CompilerParams(
            collective_id=0, has_side_effects=True, vmem_limit_bytes=VMEM_LIMIT
        ),
        name="block_backward",
    )(block_input, value_proj, gate_proj, conv_taps, norm_gain, out_proj, grad_output)
    outs = pl.pallas_call(
        write_out,
        out_shape=shapes,
        in_specs=[vmem] * 6,
        out_specs=[vmem] * 6,
        compiler_params=pltpu.CompilerParams(vmem_limit_bytes=4 * 1024 * 1024),
        name="write_out",
    )(*outs)
    return (*outs[:5], outs[5].reshape(L))


def solution(mesh):
    tp = mesh.shape["tp"]
    Y = 4
    Z = mesh.shape["sp"] // Y
    finer = Mesh(mesh.devices.reshape(Z, Y, tp // 2, 2), ("z", "y", "x", "c"))
    sp, ch = ("z", "y"), ("x", "c")
    return jax.shard_map(
        functools.partial(shards, Z, Y),
        mesh=finer,
        in_specs=(P(sp, None), P(None, ch), P(None, ch), P(None, ch), P(ch), P(None, ch), P(sp, None)),
        out_specs=(P(sp, ch), P(sp, ch), P(sp, ch), P(sp, ch), P(None, ch), P(ch)),
        check_vma=False,
    )
```

```python
import functools

import jax
import jax.numpy as jnp
from jax import lax
from jax.experimental import pallas as pl
from jax.experimental.pallas import tpu as pltpu
from jax.sharding import Mesh
from jax.sharding import PartitionSpec as P

MESH = pl.DeviceIdType.MESH
F32 = jnp.float32
BF16 = jnp.bfloat16
norm_floor = 0.1
ANYWHERE = pltpu.HBM
VMEM_LIMIT = 40 * 1024 * 1024
L = 128
S = 8
J = 16
NP = 132
HP = 164
PAD = 32
NN = 2
FAR0, NF = 3, 3
NM = 2
NO = NF + NM
NC = 4


def dot_nn(a, b):
    return lax.dot_general(a, b, (((1,), (0,)), ((), ())), preferred_element_type=F32)


def dot_nt(a, b):
    return lax.dot_general(a, b, (((1,), (1,)), ((), ())), preferred_element_type=F32)


def body(
    Z, Y, C, K,
    x_hbm, vp_hbm, gp_hbm, taps_hbm, gain_hbm, op_hbm, g_hbm,
    ig, vg, gg, og, tg, ng,
    xv, gv, wvg, wo, wg, vbuf, sbuf, slope, hist, convp, nrm, nsl, inv, act, cs, vsf, gsf, sl, slg, acc,
    tail, halo_in, halo_out, halo_back, taps, gain,
    actT, slT, wof, won, wvf, wvm, wvn, yrof, yrf, yrv, zsof, zsf, zsv, zrof, zron, zrf, zrv, zrg, ysg, yrg, yson, yron, sta, star, stb, stbr, tgs, tgy, tgzs, tgz,
    in_sem, l_sem, x_sem, g_sem, wo_ss, wo_rs, w_ss, w_rs, wy_ss, wy_rs, h_ss, h_rs, sa_ss, sa_rs, sb_ss, sb_rs, slg_ss, slg_rs,
    yof_ss, yof_rs, yon_ss, yon_rs, yf_ss, yf_rs, yv_ss, yv_rs, yg_ss, yg_rs, zof_ss, zof_rs, zon_ss, zon_rs, zf_ss, zf_rs, zv_ss, zv_rs, zg_ss, zg_rs,
    ty_ss, ty_rs, tz_ss, tz_rs,
):
    z, y, x, c = (lax.axis_index(a) for a in ("z", "y", "x", "c"))
    rows, D = xv.shape
    T = rows // S
    DB = D // 8
    DQ = DB // 4
    RB = D // (Z * Y)
    CH = rows // NC
    H = K - 1

    yn = (y + 1) % Y
    zn = (z + (y + 1) // Y) % Z
    yb = (y + Y - 1) % Y
    zb = (z + Z - 1 + (y + Y - 1) // Y) % Z
    first = (z + y) == 0
    last = (z * Y + y) == (Z * Y - 1)
    xp, xm = (x + 1) % 4, (x + 3) % 4
    xs = (x, x + 1 - 2 * (x % 2), (x + 2) % 4, 3 - x)
    cc = (c, 1 - c)

    def to(z=z, y=y, x=x, c=c):
        return {"z": z, "y": y, "x": x, "c": c}

    def remote(src, dst, ss, rs, dev):
        return pltpu.make_async_remote_copy(
            src_ref=src, dst_ref=dst, send_sem=ss, recv_sem=rs, device_id=dev, device_id_type=MESH
        )

    tp_peers = [to(x=xs[o // 2], c=cc[o % 2]) for o in range(1, 8)]
    y_peers = [to(y=(y + d) % Y) for d in range(1, Y)]
    z_peers = [to(z=(z + d) % Z) for d in range(1, Z)]
    nxt, prv = to(z=zn, y=yn), to(z=zb, y=yb)
    sent = []

    def arrived(ref, rs):
        pltpu.make_async_copy(ref, ref, rs).wait()

    def sent_all(ref, ss):
        sent.append((ref, ss))


    loads = [
        pltpu.make_async_copy(vp_hbm, wvg.at[:, pl.ds(0, L)], l_sem.at[0]),
        pltpu.make_async_copy(gp_hbm, wvg.at[:, pl.ds(L, L)], l_sem.at[0]),
        pltpu.make_async_copy(op_hbm, wo, l_sem.at[1]),
        pltpu.make_async_copy(taps_hbm, taps, l_sem.at[2]),
        pltpu.make_async_copy(gain_hbm, gain, l_sem.at[3]),
    ]
    loads[0].start()
    loads[1].start()
    XC = 4
    XR = rows // XC

    def x_load(i):
        at = pl.ds(pl.multiple_of(i * XR, XR), XR)
        return pltpu.make_async_copy(x_hbm.at[at], xv.at[at], x_sem.at[i])

    def g_load(i):
        at = pl.ds(pl.multiple_of(i * XR, XR), XR)
        return pltpu.make_async_copy(g_hbm.at[at], gv.at[at], g_sem.at[i])

    for i in (XC - 1, *range(XC - 1)):
        x_load(i).start()
    for cp in loads[2:]:
        cp.start()
    for i in range(XC):
        g_load(i).start()

    barrier = pltpu.get_barrier_semaphore()
    for dev in (*tp_peers, *y_peers):
        pl.semaphore_signal(barrier, inc=1, device_id=dev, device_id_type=MESH)
    below, above = z > 0, z < Z - 1
    into, out_of = (y == 0) & below, (y == Y - 1) & above
    for there, dev in (
        (below, to(z=(z + Z - 1) % Z)),
        (above, to(z=(z + 1) % Z)),
        (into, prv),
        (out_of, nxt),
    ):

        @pl.when(there)
        def _(dev=dev):
            pl.semaphore_signal(barrier, inc=1, device_id=dev, device_id_type=MESH)

    greeted = len(tp_peers) + len(y_peers) + sum(
        jnp.where(there, 1, 0) for there in (below, above, into, out_of)
    )

    def pass_on(k):
        n = 2**k
        for i, there, at in ((0, z + n < Z, (z + n) % Z), (1, z >= n, (z + Z - n) % Z)):

            @pl.when(there)
            def _(i=i, at=at):
                pl.semaphore_signal(in_sem.at[2 * k + i], inc=1, device_id=to(z=at), device_id_type=MESH)

    def heard(k):
        n = 2**k
        for i, there in ((0, z >= n), (1, z + n < Z)):

            @pl.when(there)
            def _(i=i):
                pl.semaphore_wait(in_sem.at[2 * k + i], 1)


    arrived(wvg, l_sem.at[0])

    right, left = to(x=xp), to(x=xm)
    partner = to(c=1 - c)

    def piece(ref, q):
        return ref.at[pl.ds(q * CH, CH)]

    def x_step(i, end):
        x_load(i).wait()
        res = dot_nn(xv[pl.ds(pl.multiple_of(i * XR, XR), XR), :], wvg[...])
        v = res[:, :L]
        s = jax.nn.sigmoid(res[:, L:])
        m = (v * s).astype(BF16).astype(F32)
        for h in range(XR // T):
            n = i * (XR // T) + h
            part = slice(h * T, (h + 1) * T)
            vbuf[pl.ds(n * NP, T), :] = v[part]
            sbuf[pl.ds(n * NP, T), :] = s[part]
            hist[pl.ds(n * HP + PAD, T), :] = m[part]
            if end and h == XR // T - 1:
                tail[...] = m[XR - PAD :]
            else:
                hist[pl.ds((n + 1) * HP, PAD), :] = m[(h + 1) * T - PAD : (h + 1) * T]

    x_step(XC - 1, True)

    def x_loop(i, carry):
        x_step(i, False)
        return carry

    pl.semaphore_wait(barrier, greeted)
    halo_m = remote(tail, halo_in, h_ss.at[0], h_rs.at[0], nxt)

    @pl.when(jnp.logical_not(last))
    def _():
        halo_m.start()

    pass_on(0)

    yq = y % 2
    y_pair = to(y=y + 1 - 2 * yq)

    def w_start(part):
        for o in range(2, 8):
            row = (xs[o // 2] * 2 + cc[o % 2]) * DB + (2 * yq + part) * DQ
            at = pl.ds(pl.multiple_of(row, DQ), DQ)
            remote(
                wvg.at[at], wg.at[o - 1, yq, part], w_ss.at[part], w_rs.at[part], tp_peers[o - 1]
            ).start()
        sent_all(wg.at[pl.ds(1, 6), yq, part], w_ss.at[part])

    def w_on(part):
        at = wg.at[pl.ds(1, 6), yq, part]
        arrived(at, w_rs.at[part])
        remote(at, at, wy_ss.at[part], wy_rs.at[part], y_pair).start()
        sent_all(at, wy_ss.at[part])

    w_start(0)
    for i in range(4):
        at = pl.ds(pl.multiple_of((xs[0] * 2 + cc[1]) * DB + i * DQ, DQ), DQ)
        remote(wvg.at[at], wg.at[0, i // 2, i % 2], wo_ss.at[0], wo_rs.at[0], tp_peers[0]).start()
    sent_all(wg.at[0], wo_ss.at[0])

    lax.fori_loop(0, XC - 1, x_loop, 0)

    for cp in loads[2:]:
        cp.wait()

    lane = lax.broadcasted_iota(jnp.int32, (S, L), 1)
    zero = jnp.zeros((S, L), F32)

    def near(ref, t):
        return ref[pl.ds(t, S, stride=NP), :]

    def wide(ref, t):
        return ref[pl.ds(t, S, stride=HP), :]

    def spread(stat, t):
        return jnp.sum(jnp.where(lane == t, stat, 0.0), axis=1, keepdims=True)

    def tap(k):
        return taps[pl.ds(k, 1), :]

    def conv_block(b, carry):
        s1, s2 = carry
        t0 = b * J
        r = [zero] * J
        for i in range(J + H):
            m = wide(hist, t0 + (PAD - H) + i)
            for j in range(J):
                k = H + j - i
                if 0 <= k < K:
                    r[j] = r[j] + tap(k) * m
        for j in range(J):
            convp[t0 + j] = r[j]
            s1 = jnp.where(lane == t0 + j, jnp.sum(r[j], axis=1, keepdims=True), s1)
            s2 = jnp.where(lane == t0 + j, jnp.sum(r[j] * r[j], axis=1, keepdims=True), s2)
        return s1, s2

    def exchange(own, got, ss, rs):
        copies = [remote(own, got.at[i], ss.at[0], rs.at[0], tp_peers[i]) for i in range(7)]
        for cp in copies:
            cp.start()
        sent_all(got, ss.at[0])

    def total(own, got, i):
        r = own[i]
        for p in range(7):
            r = r + got[p, i]
        return r * (1.0 / C)

    near_end = -(-H // J)
    s1, s2 = lax.fori_loop(near_end, T // J, conv_block, (zero, zero))

    @pl.when(first)
    def _():
        hist[pl.ds(0, PAD), :] = jnp.zeros((PAD, L), F32)

    @pl.when(jnp.logical_not(first))
    def _():
        halo_m.wait_recv()
        hist[pl.ds(0, PAD), :] = halo_in[...]

    s1, s2 = lax.fori_loop(0, near_end, conv_block, (s1, s2))
    sta[0] = s1
    sta[1] = s2
    exchange(sta, star, sa_ss, sa_rs)
    w_start(1)

    def g_loop(i, carry):
        g_load(i).wait()
        r = dot_nn(gv[pl.ds(pl.multiple_of(i * XR, XR), XR), :], wo[...])
        for h in range(XR // T):
            slope[pl.ds((i * (XR // T) + h) * NP, T), :] = r[h * T : (h + 1) * T]
        return carry

    lax.fori_loop(0, XC, g_loop, 0)

    heard(0)
    pass_on(1)

    w_on(0)

    arrived(star, sa_rs.at[0])
    center = total(sta, star, 0)
    inverse = lax.rsqrt(total(sta, star, 1) - center * center + norm_floor)
    gains = gain[...]

    def norm_block(b, carry):
        gsum, s1, s2 = carry
        t0 = b * J
        for j in range(J):
            t = t0 + j
            iv = jnp.broadcast_to(spread(inverse, t), (S, L))
            n = (convp[t] - spread(center, t)) * iv
            sc = n * gains
            sq = jax.nn.sigmoid(sc)
            act[pl.ds(t, S, stride=NP), :] = sc * sq
            ps = near(slope, t) * sq * (1.0 + sc * (1.0 - sq))
            gsum = gsum + ps * n
            ns = ps * gains
            inv[t] = iv
            nrm[t] = n
            nsl[t] = ns
            s1 = jnp.where(lane == t, jnp.sum(ns, axis=1, keepdims=True), s1)
            s2 = jnp.where(lane == t, jnp.sum(ns * n, axis=1, keepdims=True), s2)
        return gsum, s1, s2

    gsum, s1, s2 = lax.fori_loop(0, T // J, norm_block, (zero, zero, zero))
    stb[0] = s1
    stb[1] = s2
    exchange(stb, stbr, sb_ss, sb_rs)
    heard(1)
    pass_on(2)
    w_on(1)

    def flip(src, dst, row0):
        def step(n, carry):
            dst[pl.ds(row0, L), pl.ds(pl.multiple_of(n * T, T), T)] = src[pl.ds(n * NP, T), :].T.astype(BF16)
            return carry

        lax.fori_loop(0, S, step, 0)

    flip(act, actT, 0)

    def weight_block(left, right, zi, put):
        at = pl.ds(pl.multiple_of(zi * (D // Z), D // Z), D // Z)
        r = dot_nn(left[...], right[:, at]).T.astype(BF16)
        for yi in range(Y):
            put(yi, r[yi * RB : (yi + 1) * RB])

    def y_send(src, dst, ss, rs):
        for d in range(1, Y):
            remote(src.at[:, (y + d) % Y], dst.at[d - 1], ss.at[0], rs.at[0], y_peers[d - 1]).start()
        sent_all(dst, ss.at[0])

    def near_of(e):
        return (z + Z + 1 - 2 * e) % Z

    def mid_of(e):
        return (z + 2 + (Z - 4) * e) % Z

    def out_put(dst, e):
        def put(yi, r):
            dst[e, yi] = r

        return put

    def out_near_loop(e, carry):
        weight_block(actT, gv, near_of(e), out_put(won, e))
        return carry

    def out_far_loop(e, carry):
        weight_block(actT, gv, (z + 2 + e) % Z, out_put(wof, e))
        return carry

    lax.fori_loop(0, NO, out_far_loop, 0)
    weight_block(actT, gv, z, out_put(won, NN))
    lax.fori_loop(0, NN, out_near_loop, 0)

    arrived(stbr, sb_rs.at[0])
    slope_sum = total(stb, stbr, 0)
    cross_sum = total(stb, stbr, 1)

    def cs_block(b, carry):
        t0 = b * J
        for j in range(J):
            t = t0 + j
            cs[pl.ds(t, S, stride=HP), :] = inv[t] * (
                nsl[t] - spread(slope_sum, t) - nrm[t] * spread(cross_sum, t)
            )
        return carry

    lax.fori_loop(0, PAD // J, cs_block, 0)
    halo_out[...] = cs[pl.ds(0, PAD), :]
    halo_c = remote(halo_out, halo_back, h_ss.at[1], h_rs.at[1], prv)

    @pl.when(jnp.logical_not(first))
    def _():
        halo_c.start()

    y_send(wof, yrof, yof_ss, yof_rs)
    for n in range(S - 1):
        cs[pl.ds(n * HP + T, PAD), :] = cs[pl.ds((n + 1) * HP, PAD), :]
    lax.fori_loop(PAD // J, T // J, cs_block, 0)

    def slope_block(b, carry):
        t0 = b * J
        r = [zero] * J
        for i in range(J + H):
            f = wide(cs, t0 + i)
            for j in range(J):
                k = i - j
                if 0 <= k < K:
                    r[j] = r[j] + tap(k) * f
        for j in range(J):
            t = t0 + j
            s = near(sbuf, t)
            rs = r[j] * s
            vsf[pl.ds(t, S, stride=NP), :] = rs
            gsf[pl.ds(t, S, stride=NP), :] = rs * near(vbuf, t) * (1.0 - s)
        return carry

    free = (T - H) // J
    lax.fori_loop(0, free, slope_block, 0)

    def tap_block(b, sums):
        sums = list(sums)
        t0 = b * 8
        e = [wide(cs, t0 + j) for j in range(8)]
        for i in range(8 + H):
            m = wide(hist, t0 + (PAD - H) + i)
            for j in range(8):
                k = H + j - i
                if 0 <= k < K:
                    sums[k] = sums[k] + e[j] * m
        return tuple(sums)

    sums = lax.fori_loop(0, T // 8, tap_block, tuple(zero for _ in range(K)))
    for k in range(K):
        tgs[pl.ds(k, 1), :] = jnp.sum(sums[k], axis=0, keepdims=True)
    tgs[pl.ds(K, 1), :] = jnp.sum(gsum, axis=0, keepdims=True)
    for d in range(1, Y):
        remote(tgs, tgy.at[y], ty_ss.at[0], ty_rs.at[0], y_peers[d - 1]).start()
    sent_all(tgy.at[pl.ds(0, Y - 1)], ty_ss.at[0])
    tgy[y] = tgs[...]


    @pl.when(last)
    def _():
        cs[pl.ds((S - 1) * HP + T, PAD), :] = jnp.zeros((PAD, L), F32)

    @pl.when(jnp.logical_not(last))
    def _():
        halo_c.wait_recv()
        cs[pl.ds((S - 1) * HP + T, PAD), :] = halo_back[...]

    lax.fori_loop(free, T // J, slope_block, 0)

    def to_bf16(n, carry):
        at = pl.ds(pl.multiple_of(n * T, T), T)
        sl[at, pl.ds(0, L)] = vsf[pl.ds(n * NP, T), :].astype(BF16)
        sl[at, pl.ds(L, L)] = gsf[pl.ds(n * NP, T), :].astype(BF16)
        return carry

    lax.fori_loop(0, S, to_bf16, 0)

    RS = (0, 1, 5, 9, 13, 14, 15)

    def pass_slope(src, slot, q, sem, dev):
        return remote(piece(src, q), piece(slg.at[slot], q), slg_ss.at[0], sem, dev)

    def own_copy(slot, q, dev):
        return pass_slope(sl, slot, q, slg_rs.at[RS[slot] + (q if slot else 0)], dev)

    up = [own_copy(1, q, right) for q in range(NC)]
    down = [own_copy(2, q, left) for q in range(NC)]
    over = [own_copy(0, q, partner) for q in range(NC)]
    half = NC // 2
    for i in range(NC):
        up[i].start()
        down[NC - 1 - i].start()
    for i in range(NC):
        over[i].start()
    sent_all(slg, slg_ss.at[0])

    heard(2)
    for e in range(NN):
        remote(won.at[e], zron.at[e], zon_ss.at[0], zon_rs.at[0], to(z=near_of(e))).start()
    sent_all(zron, zon_ss.at[0])

    diagonal = (
        lax.broadcasted_iota(jnp.int32, (2 * L, 2 * L), 0) == lax.broadcasted_iota(jnp.int32, (2 * L, 2 * L), 1)
    ).astype(F32).astype(BF16)
    slT[...] = dot_nt(diagonal, sl[...]).astype(BF16)

    def far_loop(e, carry):
        def put(yi, r):
            wvf[e, yi] = r

        weight_block(slT, xv, (z + FAR0 + e) % Z, put)
        return carry

    def mid_loop(e, carry):
        weight_block(slT, xv, mid_of(e), out_put(wvm, e))
        return carry

    def near_send(e):
        return remote(wvn.at[e], zrg.at[e], zg_ss.at[0], zg_rs.at[0], to(z=near_of(e)))

    def near_loop(e, carry):
        weight_block(slT, xv, near_of(e), out_put(wvn, e))
        near_send(e).start()
        return carry

    lax.fori_loop(0, NF, far_loop, 0)
    y_send(wvf, yrf, yf_ss, yf_rs)
    lax.fori_loop(0, NN, near_loop, 0)
    sent_all(zrg, zg_ss.at[0])
    lax.fori_loop(0, NM, mid_loop, 0)
    y_send(wvm, yrv, yv_ss, yv_rs)
    weight_block(slT, xv, z, out_put(wvn, NN))

    def weights_from(slot):
        core = 1 if slot == 0 or slot > 3 else 0
        base = slot if slot <= 3 else slot - 3
        if base == 0:
            return wg[0].reshape(DB, 2 * L)
        if base == 3:
            return wg[3 + core].reshape(DB, 2 * L)
        way = 3 - 2 * (x % 2) if base == 1 else 1 + 2 * (x % 2)
        return wg[2 * way + core - 1].reshape(DB, 2 * L)

    at = pl.ds(pl.multiple_of((x * 2 + c) * DB, DB), DB)
    acc[...] = dot_nt(sl[...], wvg[at, :])

    def add(slot, q):
        at = pl.ds(q * CH, CH)
        acc[at, :] += dot_nt(slg[slot, at, :], weights_from(slot))

    def pf(slot, q):
        sem = slg_rs.at[RS[slot + 3] + (q if slot == 3 else 0)]
        cp = pass_slope(slg.at[slot], slot + 3, q, sem, partner)
        cp.start()
        return cp

    def near_sum(own, got, z_rs, ys, yr, y_ss, y_rs):
        arrived(got, z_rs.at[0])
        for yi in range(Y):
            r = own[NN, yi].astype(F32)
            for e in range(NN):
                r = r + got[e, yi].astype(F32)
            ys[yi] = r.astype(BF16)
        for d in range(1, Y):
            remote(ys.at[(y + d) % Y], yr.at[d - 1], y_ss.at[0], y_rs.at[0], y_peers[d - 1]).start()
        sent_all(yr, y_ss.at[0])

    fwd = {}
    pfs = {}

    def take(i):
        for slot, q, copies, way in ((1, i, up, right), (2, NC - 1 - i, down, left)):
            copies[q].wait_recv()
            if i < half:
                fwd[q] = pass_slope(slg.at[slot], 3, q, slg_rs.at[RS[3] + q], way)
                fwd[q].start()
            pfs[slot, q] = pf(slot, q)

    def use(i):
        add(0, i)
        add(1, i)
        add(2, NC - 1 - i)

    take(0)
    arrived(tgy.at[pl.ds(0, Y - 1)], ty_rs.at[0])
    t = tgy[0]
    for yi in range(1, Y):
        t = t + tgy[yi]
    tgzs[...] = t.astype(BF16)
    tgz[z] = t.astype(BF16)
    for d in range(1, Z):
        remote(tgzs, tgz.at[z], tz_ss.at[0], tz_rs.at[0], z_peers[d - 1]).start()
    sent_all(tgz.at[pl.ds(0, Z - 1)], tz_ss.at[0])
    arrived(yrof, yof_rs.at[0])
    for e in range(NO):
        r = wof[e, y].astype(F32)
        for d in range(Y - 1):
            r = r + yrof[d, e].astype(F32)
        zsof[e] = r.astype(BF16)
        remote(zsof.at[e], zrof.at[e], zof_ss.at[0], zof_rs.at[0], to(z=(z + 2 + e) % Z)).start()
    sent_all(zrof, zof_ss.at[0])
    near_sum(won, zron, zon_rs, yson, yron, yon_ss, yon_rs)
    take(1)
    arrived(yrf, yf_rs.at[0])
    for e in range(NF):
        r = wvf[e, y].astype(F32)
        for d in range(Y - 1):
            r = r + yrf[d, e].astype(F32)
        zsf[e] = r.astype(BF16)
        remote(zsf.at[e], zrf.at[e], zf_ss.at[0], zf_rs.at[0], to(z=(z + FAR0 + e) % Z)).start()
    sent_all(zrf, zf_ss.at[0])
    arrived(slg.at[0], slg_rs.at[RS[0]])
    arrived(wg.at[0], wo_rs.at[0])
    for part in range(2):
        arrived(wg.at[pl.ds(1, 6), 1 - yq, part], wy_rs.at[part])
    use(0)
    take(2)
    arrived(yrv, yv_rs.at[0])
    for e in range(NM):
        r = wvm[e, y].astype(F32)
        for d in range(Y - 1):
            r = r + yrv[d, e].astype(F32)
        zsv[e] = r.astype(BF16)
        remote(zsv.at[e], zrv.at[e], zv_ss.at[0], zv_rs.at[0], to(z=mid_of(e))).start()
    sent_all(zrv, zv_ss.at[0])
    take(3)
    use(1)
    use(2)
    use(3)
    near_sum(wvn, zrg, zg_rs, ysg, yrg, yg_ss, yg_rs)
    for slot in (4, 5):
        arrived(slg.at[slot], slg_rs.at[RS[slot]])
        for q in range(NC):
            add(slot, q)

    order = [q for i in range(half) for q in (i, NC - 1 - i)]
    for q in order:
        fwd[q].wait_recv()
        pfs[3, q] = pf(3, q)
        add(3, q)
    for q in order:
        pfs[3, q].wait_recv()
        add(6, q)
    ig[...] = acc[...].astype(BF16)

    arrived(zrof, zof_rs.at[0])
    arrived(yron, yon_rs.at[0])
    r = yson[y].astype(F32)
    for d in range(Y - 1):
        r = r + yron[d].astype(F32)
    for e in range(NO):
        r = r + zrof[e].astype(F32)
    og[...] = r
    arrived(tgz.at[pl.ds(0, Z - 1)], tz_rs.at[0])
    t = tgz[0].astype(F32)
    for zi in range(1, Z):
        t = t + tgz[zi].astype(F32)
    tg[...] = t[:K]
    ng[...] = t[K : K + 1]
    arrived(zrf, zf_rs.at[0])
    arrived(zrv, zv_rs.at[0])
    arrived(yrg, yg_rs.at[0])
    r = ysg[y].astype(F32)
    for got, count in ((yrg, Y - 1), (zrf, NF), (zrv, NM)):
        for e in range(count):
            r = r + got[e].astype(F32)
    vg[...] = r[:, :L]
    gg[...] = r[:, L:]

    for ref, ss in sent:
        arrived(ref, ss)

    @pl.when(jnp.logical_not(last))
    def _():
        halo_m.wait_send()

    @pl.when(jnp.logical_not(first))
    def _():
        halo_c.wait_send()


def write_out(*refs):
    half = len(refs) // 2
    for src, dst in zip(refs[:half], refs[half:]):
        dst[...] = src[...]


def shards(Z, Y, block_input, value_proj, gate_proj, conv_taps, norm_gain, out_proj, grad_output):
    rows, D = block_input.shape
    K = conv_taps.shape[0]
    C = value_proj.shape[1] * 8
    DB, RB, T = D // 8, D // (Z * Y), rows // S
    vm = pltpu.VMEM
    dma = pltpu.SemaphoreType.DMA
    hbm, vmem = pl.BlockSpec(memory_space=ANYWHERE), pl.BlockSpec(memory_space=pltpu.VMEM)
    near, wide = vm((S * NP, L), F32), vm((S * HP, L), F32)
    flat = vm((T, S, L), F32)
    halo = vm((PAD, L), F32)
    stat, stats = vm((2, S, L), F32), vm((7, 2, S, L), F32)
    scratch = [
        vm((rows, D), BF16), vm((rows, D), BF16), vm((D, 2 * L), BF16), vm((D, L), BF16), vm((7, 2, 2, DB // 4, 2 * L), BF16),
        near, near, near, wide, flat, flat, flat, flat, near, wide,
        near, near, vm((rows, 2 * L), BF16), vm((7, rows, 2 * L), BF16), vm((rows, DB), F32),
        halo, halo, halo, halo, vm((K, L), F32), vm((1, L), F32),
        vm((L, rows), BF16), vm((2 * L, rows), BF16),
        vm((NO, Y, RB, L), BF16), vm((NN + 1, Y, RB, L), BF16),
        vm((NF, Y, RB, 2 * L), BF16), vm((NM, Y, RB, 2 * L), BF16), vm((NN + 1, Y, RB, 2 * L), BF16),
        vm((Y - 1, NO, RB, L), BF16), vm((Y - 1, NF, RB, 2 * L), BF16), vm((Y - 1, NM, RB, 2 * L), BF16),
        vm((NO, RB, L), BF16), vm((NF, RB, 2 * L), BF16), vm((NM, RB, 2 * L), BF16),
        vm((NO, RB, L), BF16), vm((NN, Y, RB, L), BF16), vm((NF, RB, 2 * L), BF16), vm((NM, RB, 2 * L), BF16),
        vm((NN, Y, RB, 2 * L), BF16), vm((Y, RB, 2 * L), BF16), vm((Y - 1, RB, 2 * L), BF16),
        vm((Y, RB, L), BF16), vm((Y - 1, RB, L), BF16),
        stat, stats, stat, stats,
        halo, vm((Y, PAD, L), F32), vm((PAD, L), BF16), vm((Z, PAD, L), BF16),
        pltpu.SemaphoreType.REGULAR((6,)),
        dma((4,)), dma((4,)), dma((4,)), *[dma((1,)) for _ in range(2)], *[dma((2,)) for _ in range(6)],
        *[dma((1,)) for _ in range(4)], dma((1,)), dma((19,)), *[dma((1,)) for _ in range(24)],
    ]
    shapes = (
        jax.ShapeDtypeStruct((rows, DB), BF16),
        jax.ShapeDtypeStruct((RB, L), F32),
        jax.ShapeDtypeStruct((RB, L), F32),
        jax.ShapeDtypeStruct((RB, L), F32),
        jax.ShapeDtypeStruct((K, L), F32),
        jax.ShapeDtypeStruct((1, L), F32),
    )
    norm_gain = norm_gain.reshape(1, L)
    block_input, value_proj, gate_proj, conv_taps, norm_gain, out_proj, grad_output = (
        pltpu.with_memory_space_constraint(a, pltpu.HBM)
        for a in (block_input, value_proj, gate_proj, conv_taps, norm_gain, out_proj, grad_output)
    )
    outs = pl.pallas_call(
        functools.partial(body, Z, Y, C, K),
        out_shape=shapes,
        in_specs=[hbm] * 7,
        out_specs=[vmem] * 6,
        scratch_shapes=scratch,
        compiler_params=pltpu.CompilerParams(
            collective_id=0, has_side_effects=True, vmem_limit_bytes=VMEM_LIMIT
        ),
        name="block_backward",
    )(block_input, value_proj, gate_proj, conv_taps, norm_gain, out_proj, grad_output)
    outs = pl.pallas_call(
        write_out,
        out_shape=shapes,
        in_specs=[vmem] * 6,
        out_specs=[vmem] * 6,
        compiler_params=pltpu.CompilerParams(vmem_limit_bytes=4 * 1024 * 1024),
        name="write_out",
    )(*outs)
    return (*outs[:5], outs[5].reshape(L))


def solution(mesh):
    tp = mesh.shape["tp"]
    Y = 4
    Z = mesh.shape["sp"] // Y
    finer = Mesh(mesh.devices.reshape(Z, Y, tp // 2, 2), ("z", "y", "x", "c"))
    sp, ch = ("z", "y"), ("x", "c")
    return jax.shard_map(
        functools.partial(shards, Z, Y),
        mesh=finer,
        in_specs=(P(sp, None), P(None, ch), P(None, ch), P(None, ch), P(ch), P(None, ch), P(sp, None)),
        out_specs=(P(sp, ch), P(sp, ch), P(sp, ch), P(sp, ch), P(None, ch), P(ch)),
        check_vma=False,
    )
```

```python
import functools

import jax
import jax.numpy as jnp
from jax import lax
from jax.experimental import pallas as pl
from jax.experimental.pallas import tpu as pltpu
from jax.sharding import Mesh
from jax.sharding import PartitionSpec as P

MESH = pl.DeviceIdType.MESH
F32 = jnp.float32
BF16 = jnp.bfloat16
norm_floor = 0.1
ANYWHERE = pltpu.HBM
VMEM_LIMIT = 40 * 1024 * 1024
L = 128
S = 8
J = 16
NP = 132
HP = 164
PAD = 32
NN = 2
FAR0, NF = 3, 3
NM = 2
NO = NF + NM
NC = 4
EARLY = (0, 3)


def dot_nn(a, b):
    return lax.dot_general(a, b, (((1,), (0,)), ((), ())), preferred_element_type=F32)


def dot_nt(a, b):
    return lax.dot_general(a, b, (((1,), (1,)), ((), ())), preferred_element_type=F32)


def body(
    Z, Y, C, K,
    x_hbm, vp_hbm, gp_hbm, taps_hbm, gain_hbm, op_hbm, g_hbm,
    ig, vg, gg, og, tg, ng,
    xv, gv, wvg, wo, wg, vbuf, sbuf, slope, hist, convp, nrm, nsl, inv, act, cs, vsf, gsf, sl, slg, acc,
    sqb, er, msf, msl, mr, tail, halo_in, halo_out, halo_back, taps, gain,
    actT, slT, wof, won, wvf, wvm, wvn, yrof, yrf, yrv, zsof, zsf, zsv, zrof, zron, zrf, zrv, zrg, ysg, yrg, yson, yron, sta, star, stb, stbr, tgs, tgy, tgzs, tgz,
    in_sem, l_sem, x_sem, g_sem, wo_ss, wo_rs, w_ss, w_rs, wy_ss, wy_rs, h_ss, h_rs, sa_ss, sa_rs, sb_ss, sb_rs, slg_ss, slg_rs, mr_rs, er_ss, er_rs,
    yof_ss, yof_rs, yon_ss, yon_rs, yf_ss, yf_rs, yv_ss, yv_rs, yg_ss, yg_rs, zof_ss, zof_rs, zon_ss, zon_rs, zf_ss, zf_rs, zv_ss, zv_rs, zg_ss, zg_rs,
    ty_ss, ty_rs, tz_ss, tz_rs,
):
    z, y, x, c = (lax.axis_index(a) for a in ("z", "y", "x", "c"))
    rows, D = xv.shape
    T = rows // S
    DB = D // 8
    DQ = DB // 4
    RB = D // (Z * Y)
    CH = rows // NC
    H = K - 1

    yn = (y + 1) % Y
    zn = (z + (y + 1) // Y) % Z
    yb = (y + Y - 1) % Y
    zb = (z + Z - 1 + (y + Y - 1) // Y) % Z
    first = (z + y) == 0
    last = (z * Y + y) == (Z * Y - 1)
    xp, xm = (x + 1) % 4, (x + 3) % 4
    xs = (x, x + 1 - 2 * (x % 2), (x + 2) % 4, 3 - x)
    cc = (c, 1 - c)

    def to(z=z, y=y, x=x, c=c):
        return {"z": z, "y": y, "x": x, "c": c}

    def remote(src, dst, ss, rs, dev):
        return pltpu.make_async_remote_copy(
            src_ref=src, dst_ref=dst, send_sem=ss, recv_sem=rs, device_id=dev, device_id_type=MESH
        )

    tp_peers = [to(x=xs[o // 2], c=cc[o % 2]) for o in range(1, 8)]
    y_peers = [to(y=(y + d) % Y) for d in range(1, Y)]
    z_peers = [to(z=(z + d) % Z) for d in range(1, Z)]
    nxt, prv = to(z=zn, y=yn), to(z=zb, y=yb)
    sent = []

    def arrived(ref, rs):
        pltpu.make_async_copy(ref, ref, rs).wait()

    def sent_all(ref, ss):
        sent.append((ref, ss))


    loads = [
        pltpu.make_async_copy(vp_hbm, wvg.at[:, pl.ds(0, L)], l_sem.at[0]),
        pltpu.make_async_copy(gp_hbm, wvg.at[:, pl.ds(L, L)], l_sem.at[0]),
        pltpu.make_async_copy(op_hbm, wo, l_sem.at[1]),
        pltpu.make_async_copy(taps_hbm, taps, l_sem.at[2]),
        pltpu.make_async_copy(gain_hbm, gain, l_sem.at[3]),
    ]
    loads[0].start()
    loads[1].start()
    XC = 4
    XR = rows // XC

    def x_load(i):
        at = pl.ds(pl.multiple_of(i * XR, XR), XR)
        return pltpu.make_async_copy(x_hbm.at[at], xv.at[at], x_sem.at[i])

    def g_load(i):
        at = pl.ds(pl.multiple_of(i * XR, XR), XR)
        return pltpu.make_async_copy(g_hbm.at[at], gv.at[at], g_sem.at[i])

    for i in (XC - 1, *range(XC - 1)):
        x_load(i).start()
    for cp in loads[2:]:
        cp.start()
    for i in range(XC):
        g_load(i).start()

    barrier = pltpu.get_barrier_semaphore()
    for dev in (*tp_peers, *y_peers):
        pl.semaphore_signal(barrier, inc=1, device_id=dev, device_id_type=MESH)
    below, above = z > 0, z < Z - 1
    into, out_of = (y == 0) & below, (y == Y - 1) & above
    for there, dev in (
        (below, to(z=(z + Z - 1) % Z)),
        (above, to(z=(z + 1) % Z)),
        (into, prv),
        (out_of, nxt),
    ):

        @pl.when(there)
        def _(dev=dev):
            pl.semaphore_signal(barrier, inc=1, device_id=dev, device_id_type=MESH)

    greeted = len(tp_peers) + len(y_peers) + sum(
        jnp.where(there, 1, 0) for there in (below, above, into, out_of)
    )

    def pass_on(k):
        n = 2**k
        for i, there, at in ((0, z + n < Z, (z + n) % Z), (1, z >= n, (z + Z - n) % Z)):

            @pl.when(there)
            def _(i=i, at=at):
                pl.semaphore_signal(in_sem.at[2 * k + i], inc=1, device_id=to(z=at), device_id_type=MESH)

    def heard(k):
        n = 2**k
        for i, there in ((0, z >= n), (1, z + n < Z)):

            @pl.when(there)
            def _(i=i):
                pl.semaphore_wait(in_sem.at[2 * k + i], 1)


    arrived(wvg, l_sem.at[0])

    right, left = to(x=xp), to(x=xm)
    partner = to(c=1 - c)

    def piece(ref, q):
        return ref.at[pl.ds(q * CH, CH)]

    def early_own(k):
        src = piece(sqb, EARLY[k])
        return [
            remote(src, er.at[0, k], er_ss.at[0], er_rs.at[k], right),
            remote(src, er.at[1, k], er_ss.at[0], er_rs.at[2 + k], left),
        ]

    def early_on(k):
        return remote(er.at[k, k], er.at[2, k], er_ss.at[0], er_rs.at[4 + k], (right, left)[k])

    def early_over(i, k):
        return remote(er.at[i, k], er.at[i + 3, k], er_ss.at[0], er_rs.at[6 + 2 * i + k], partner)

    def early_arrived(i, k):
        arrived(er.at[i, k], er_rs.at[2 * i + k])

    def x_step(i, end):
        x_load(i).wait()
        res = dot_nn(xv[pl.ds(pl.multiple_of(i * XR, XR), XR), :], wvg[...])
        v = res[:, :L]
        s = jax.nn.sigmoid(res[:, L:])
        m = (v * s).astype(BF16).astype(F32)
        for h in range(XR // T):
            n = i * (XR // T) + h
            part = slice(h * T, (h + 1) * T)
            vbuf[pl.ds(n * NP, T), :] = v[part]
            sbuf[pl.ds(n * NP, T), :] = s[part]
            at = pl.ds(pl.multiple_of(n * T, T), T)
            sqb[at, pl.ds(0, L)] = s[part].astype(BF16)
            sqb[at, pl.ds(L, L)] = (v[part] * s[part] * (1.0 - s[part])).astype(BF16)
            hist[pl.ds(n * HP + PAD, T), :] = m[part]
            if end and h == XR // T - 1:
                tail[...] = m[XR - PAD :]
            else:
                hist[pl.ds((n + 1) * HP, PAD), :] = m[(h + 1) * T - PAD : (h + 1) * T]

    x_step(XC - 1, True)

    def x_loop(i, carry):
        x_step(i, False)
        return carry

    pl.semaphore_wait(barrier, greeted)
    halo_m = remote(tail, halo_in, h_ss.at[0], h_rs.at[0], nxt)

    @pl.when(jnp.logical_not(last))
    def _():
        halo_m.start()

    pass_on(0)

    yq = y % 2
    y_pair = to(y=y + 1 - 2 * yq)

    def w_start(part):
        for o in range(2, 8):
            row = (xs[o // 2] * 2 + cc[o % 2]) * DB + (2 * yq + part) * DQ
            at = pl.ds(pl.multiple_of(row, DQ), DQ)
            remote(
                wvg.at[at], wg.at[o - 1, yq, part], w_ss.at[part], w_rs.at[part], tp_peers[o - 1]
            ).start()
        sent_all(wg.at[pl.ds(1, 6), yq, part], w_ss.at[part])

    def w_on(part):
        at = wg.at[pl.ds(1, 6), yq, part]
        arrived(at, w_rs.at[part])
        remote(at, at, wy_ss.at[part], wy_rs.at[part], y_pair).start()
        sent_all(at, wy_ss.at[part])

    w_start(0)
    for i in range(4):
        at = pl.ds(pl.multiple_of((xs[0] * 2 + cc[1]) * DB + i * DQ, DQ), DQ)
        remote(wvg.at[at], wg.at[0, i // 2, i % 2], wo_ss.at[0], wo_rs.at[0], tp_peers[0]).start()
    sent_all(wg.at[0], wo_ss.at[0])

    lax.fori_loop(0, XC - 1, x_loop, 0)

    for cp in loads[2:]:
        cp.wait()

    lane = lax.broadcasted_iota(jnp.int32, (S, L), 1)
    zero = jnp.zeros((S, L), F32)

    def near(ref, t):
        return ref[pl.ds(t, S, stride=NP), :]

    def wide(ref, t):
        return ref[pl.ds(t, S, stride=HP), :]

    def spread(stat, t):
        return jnp.sum(jnp.where(lane == t, stat, 0.0), axis=1, keepdims=True)

    def tap(k):
        return taps[pl.ds(k, 1), :]

    def conv_block(b, carry):
        s1, s2 = carry
        t0 = b * J
        r = [zero] * J
        for i in range(J + H):
            m = wide(hist, t0 + (PAD - H) + i)
            for j in range(J):
                k = H + j - i
                if 0 <= k < K:
                    r[j] = r[j] + tap(k) * m
        for j in range(J):
            convp[t0 + j] = r[j]
            s1 = jnp.where(lane == t0 + j, jnp.sum(r[j], axis=1, keepdims=True), s1)
            s2 = jnp.where(lane == t0 + j, jnp.sum(r[j] * r[j], axis=1, keepdims=True), s2)
        return s1, s2

    def exchange(own, got, ss, rs):
        copies = [remote(own, got.at[i], ss.at[0], rs.at[0], tp_peers[i]) for i in range(7)]
        for cp in copies:
            cp.start()
        sent_all(got, ss.at[0])

    def total(own, got, i):
        r = own[i]
        for p in range(7):
            r = r + got[p, i]
        return r * (1.0 / C)

    near_end = -(-H // J)
    s1, s2 = lax.fori_loop(near_end, T // J, conv_block, (zero, zero))

    @pl.when(first)
    def _():
        hist[pl.ds(0, PAD), :] = jnp.zeros((PAD, L), F32)

    @pl.when(jnp.logical_not(first))
    def _():
        halo_m.wait_recv()
        hist[pl.ds(0, PAD), :] = halo_in[...]

    s1, s2 = lax.fori_loop(0, near_end, conv_block, (s1, s2))
    sta[0] = s1
    sta[1] = s2
    exchange(sta, star, sa_ss, sa_rs)
    w_start(1)
    for cp in early_own(1):
        cp.start()

    def g_loop(i, carry):
        g_load(i).wait()
        r = dot_nn(gv[pl.ds(pl.multiple_of(i * XR, XR), XR), :], wo[...])
        for h in range(XR // T):
            slope[pl.ds((i * (XR // T) + h) * NP, T), :] = r[h * T : (h + 1) * T]
        return carry

    lax.fori_loop(0, XC, g_loop, 0)

    heard(0)
    pass_on(1)

    w_on(0)

    arrived(star, sa_rs.at[0])
    center = total(sta, star, 0)
    inverse = lax.rsqrt(total(sta, star, 1) - center * center + norm_floor)
    gains = gain[...]

    def norm_block(b, carry):
        gsum, s1, s2 = carry
        t0 = b * J
        for j in range(J):
            t = t0 + j
            iv = jnp.broadcast_to(spread(inverse, t), (S, L))
            n = (convp[t] - spread(center, t)) * iv
            sc = n * gains
            sq = jax.nn.sigmoid(sc)
            act[pl.ds(t, S, stride=NP), :] = sc * sq
            ps = near(slope, t) * sq * (1.0 + sc * (1.0 - sq))
            gsum = gsum + ps * n
            ns = ps * gains
            inv[t] = iv
            nrm[t] = n
            nsl[t] = ns
            s1 = jnp.where(lane == t, jnp.sum(ns, axis=1, keepdims=True), s1)
            s2 = jnp.where(lane == t, jnp.sum(ns * n, axis=1, keepdims=True), s2)
        return gsum, s1, s2

    gsum, s1, s2 = lax.fori_loop(0, T // J, norm_block, (zero, zero, zero))
    stb[0] = s1
    stb[1] = s2
    exchange(stb, stbr, sb_ss, sb_rs)
    heard(1)
    pass_on(2)
    for cp in early_own(0):
        cp.start()
    w_on(1)

    def flip(src, dst, row0):
        def step(n, carry):
            dst[pl.ds(row0, L), pl.ds(pl.multiple_of(n * T, T), T)] = src[pl.ds(n * NP, T), :].T.astype(BF16)
            return carry

        lax.fori_loop(0, S, step, 0)

    flip(act, actT, 0)

    def weight_block(left, right, zi, put):
        at = pl.ds(pl.multiple_of(zi * (D // Z), D // Z), D // Z)
        r = dot_nn(left[...], right[:, at]).T.astype(BF16)
        for yi in range(Y):
            put(yi, r[yi * RB : (yi + 1) * RB])

    def y_send(src, dst, ss, rs):
        for d in range(1, Y):
            remote(src.at[:, (y + d) % Y], dst.at[d - 1], ss.at[0], rs.at[0], y_peers[d - 1]).start()
        sent_all(dst, ss.at[0])

    def near_of(e):
        return (z + Z + 1 - 2 * e) % Z

    def mid_of(e):
        return (z + 2 + (Z - 4) * e) % Z

    def out_put(dst, e):
        def put(yi, r):
            dst[e, yi] = r

        return put

    def out_near_loop(e, carry):
        weight_block(actT, gv, near_of(e), out_put(won, e))
        return carry

    def out_far_loop(e, carry):
        weight_block(actT, gv, (z + 2 + e) % Z, out_put(wof, e))
        return carry

    lax.fori_loop(0, NO, out_far_loop, 0)
    weight_block(actT, gv, z, out_put(won, NN))
    lax.fori_loop(0, NN, out_near_loop, 0)

    for i in range(2):
        early_arrived(i, 1)
        early_over(i, 1).start()
    early_on(1).start()

    arrived(stbr, sb_rs.at[0])
    slope_sum = total(stb, stbr, 0)
    cross_sum = total(stb, stbr, 1)

    def cs_block(b, carry):
        t0 = b * J
        for j in range(J):
            t = t0 + j
            cs[pl.ds(t, S, stride=HP), :] = inv[t] * (
                nsl[t] - spread(slope_sum, t) - nrm[t] * spread(cross_sum, t)
            )
        return carry

    lax.fori_loop(0, PAD // J, cs_block, 0)
    halo_out[...] = cs[pl.ds(0, PAD), :]
    halo_c = remote(halo_out, halo_back, h_ss.at[1], h_rs.at[1], prv)

    @pl.when(jnp.logical_not(first))
    def _():
        halo_c.start()

    y_send(wof, yrof, yof_ss, yof_rs)
    for n in range(S - 1):
        cs[pl.ds(n * HP + T, PAD), :] = cs[pl.ds((n + 1) * HP, PAD), :]
    lax.fori_loop(PAD // J, T // J, cs_block, 0)

    def slope_block(b, carry):
        t0 = b * J
        r = [zero] * J
        for i in range(J + H):
            f = wide(cs, t0 + i)
            for j in range(J):
                k = i - j
                if 0 <= k < K:
                    r[j] = r[j] + tap(k) * f
        for j in range(J):
            t = t0 + j
            s = near(sbuf, t)
            msf[pl.ds(t, S, stride=NP), :] = r[j]
            rs = r[j] * s
            vsf[pl.ds(t, S, stride=NP), :] = rs
            gsf[pl.ds(t, S, stride=NP), :] = rs * near(vbuf, t) * (1.0 - s)
        return carry

    free = (T - H) // J
    lax.fori_loop(0, free, slope_block, 0)

    def tap_block(b, sums):
        sums = list(sums)
        t0 = b * 8
        e = [wide(cs, t0 + j) for j in range(8)]
        for i in range(8 + H):
            m = wide(hist, t0 + (PAD - H) + i)
            for j in range(8):
                k = H + j - i
                if 0 <= k < K:
                    sums[k] = sums[k] + e[j] * m
        return tuple(sums)

    for i in range(2):
        early_arrived(i, 0)
        early_over(i, 0).start()
    early_on(0).start()
    sent_all(er, er_ss.at[0])

    sums = lax.fori_loop(0, T // 8, tap_block, tuple(zero for _ in range(K)))
    for k in range(K):
        tgs[pl.ds(k, 1), :] = jnp.sum(sums[k], axis=0, keepdims=True)
    tgs[pl.ds(K, 1), :] = jnp.sum(gsum, axis=0, keepdims=True)
    for d in range(1, Y):
        remote(tgs, tgy.at[y], ty_ss.at[0], ty_rs.at[0], y_peers[d - 1]).start()
    sent_all(tgy.at[pl.ds(0, Y - 1)], ty_ss.at[0])
    tgy[y] = tgs[...]


    @pl.when(last)
    def _():
        cs[pl.ds((S - 1) * HP + T, PAD), :] = jnp.zeros((PAD, L), F32)

    @pl.when(jnp.logical_not(last))
    def _():
        halo_c.wait_recv()
        cs[pl.ds((S - 1) * HP + T, PAD), :] = halo_back[...]

    lax.fori_loop(free, T // J, slope_block, 0)

    def to_bf16(n, carry):
        at = pl.ds(pl.multiple_of(n * T, T), T)
        msl[at, :] = msf[pl.ds(n * NP, T), :].astype(BF16)
        sl[at, pl.ds(0, L)] = vsf[pl.ds(n * NP, T), :].astype(BF16)
        sl[at, pl.ds(L, L)] = gsf[pl.ds(n * NP, T), :].astype(BF16)
        return carry

    lax.fori_loop(0, S, to_bf16, 0)

    RS = (0, 1, 5, 9, 13, 14, 15)

    def held(slot, q):
        return mr.at[slot - 1, EARLY.index(q)] if q in EARLY else piece(slg.at[slot], q)

    def pass_slope(src, slot, q, sem, dev):
        return remote(src, held(slot, q), slg_ss.at[1 if q in EARLY else 0], sem, dev)

    def own_copy(slot, q, dev):
        return pass_slope(piece(msl if q in EARLY else sl, q), slot, q, slg_rs.at[RS[slot] + q], dev)

    up = [own_copy(1, q, right) for q in range(NC)]
    down = [own_copy(2, q, left) for q in range(NC)]
    over = [remote(piece(sl, q), piece(slg.at[0], q), slg_ss.at[0], slg_rs.at[0], partner) for q in range(NC)]
    half = NC // 2
    for i in range(NC):
        up[i].start()
        down[NC - 1 - i].start()
    for i in range(NC):
        over[i].start()
    sent_all(slg.at[pl.ds(0, 4)], slg_ss.at[0])
    sent_all(mr, slg_ss.at[1])

    heard(2)
    for e in range(NN):
        remote(won.at[e], zron.at[e], zon_ss.at[0], zon_rs.at[0], to(z=near_of(e))).start()
    sent_all(zron, zon_ss.at[0])
    diagonal = (
        lax.broadcasted_iota(jnp.int32, (2 * L, 2 * L), 0) == lax.broadcasted_iota(jnp.int32, (2 * L, 2 * L), 1)
    ).astype(F32).astype(BF16)
    slT[...] = dot_nt(diagonal, sl[...]).astype(BF16)

    def far_of(e):
        return (z + FAR0 + 1 - e % 2 + e // 2) % Z

    def far_loop(e, carry):
        def put(yi, r):
            wvf[e, yi] = r

        weight_block(slT, xv, far_of(e), put)
        for d in range(1, Y):
            remote(
                wvf.at[e, (y + d) % Y], yrf.at[d - 1, e], yf_ss.at[0], yf_rs.at[e], y_peers[d - 1]
            ).start()
        return carry

    def mid_loop(e, carry):
        weight_block(slT, xv, mid_of(e), out_put(wvm, e))
        return carry

    def near_send(e):
        return remote(wvn.at[e], zrg.at[e], zg_ss.at[0], zg_rs.at[0], to(z=near_of(e)))

    def near_loop(e, carry):
        weight_block(slT, xv, near_of(e), out_put(wvn, e))
        near_send(e).start()
        return carry

    lax.fori_loop(0, NF, far_loop, 0)
    sent_all(yrf, yf_ss.at[0])
    lax.fori_loop(0, NN, near_loop, 0)
    sent_all(zrg, zg_ss.at[0])
    lax.fori_loop(0, NM, mid_loop, 0)
    y_send(wvm, yrv, yv_ss, yv_rs)
    weight_block(slT, xv, z, out_put(wvn, NN))

    def weights_from(slot):
        core = 1 if slot == 0 or slot > 3 else 0
        base = slot if slot <= 3 else slot - 3
        if base == 0:
            return wg[0].reshape(DB, 2 * L)
        if base == 3:
            return wg[3 + core].reshape(DB, 2 * L)
        way = 3 - 2 * (x % 2) if base == 1 else 1 + 2 * (x % 2)
        return wg[2 * way + core - 1].reshape(DB, 2 * L)

    at = pl.ds(pl.multiple_of((x * 2 + c) * DB, DB), DB)
    acc[...] = dot_nt(sl[...], wvg[at, :])

    def add(slot, q):
        at = pl.ds(q * CH, CH)
        if slot and q in EARLY:
            k = EARLY.index(q)
            m = mr[slot - 1, k].astype(F32)
            f = er[slot - 1, k].astype(F32)
            block = jnp.concatenate([m * f[:, :L], m * f[:, L:]], axis=1).astype(BF16)
        else:
            block = slg[slot, at, :]
        acc[at, :] += dot_nt(block, weights_from(slot))

    def pf(slot, q):
        if slot == 3:
            sem = slg_rs.at[RS[6] + q]
        else:
            sem = mr_rs.at[slot - 1] if q in EARLY else slg_rs.at[RS[slot + 3]]
        cp = pass_slope(held(slot, q), slot + 3, q, sem, partner)
        cp.start()
        return cp

    def near_sum(own, got, z_rs, ys, yr, y_ss, y_rs):
        arrived(got, z_rs.at[0])
        for yi in range(Y):
            r = own[NN, yi].astype(F32)
            for e in range(NN):
                r = r + got[e, yi].astype(F32)
            ys[yi] = r.astype(BF16)
        for d in range(1, Y):
            remote(ys.at[(y + d) % Y], yr.at[d - 1], y_ss.at[0], y_rs.at[0], y_peers[d - 1]).start()
        sent_all(yr, y_ss.at[0])

    fwd = {}
    pfs = {}

    def take(i):
        for slot, q, copies, way in ((1, i, up, right), (2, NC - 1 - i, down, left)):
            copies[q].wait_recv()
            if i < half:
                fwd[q] = pass_slope(held(slot, q), 3, q, slg_rs.at[RS[3] + q], way)
                fwd[q].start()
            pfs[slot, q] = pf(slot, q)

    def use(i):
        add(0, i)
        add(1, i)
        add(2, NC - 1 - i)

    take(0)
    early_arrived(2, 1)
    early_over(2, 1).start()
    arrived(tgy.at[pl.ds(0, Y - 1)], ty_rs.at[0])
    t = tgy[0]
    for yi in range(1, Y):
        t = t + tgy[yi]
    tgzs[...] = t.astype(BF16)
    tgz[z] = t.astype(BF16)
    for d in range(1, Z):
        remote(tgzs, tgz.at[z], tz_ss.at[0], tz_rs.at[0], z_peers[d - 1]).start()
    sent_all(tgz.at[pl.ds(0, Z - 1)], tz_ss.at[0])
    arrived(yrof, yof_rs.at[0])
    for e in range(NO):
        r = wof[e, y].astype(F32)
        for d in range(Y - 1):
            r = r + yrof[d, e].astype(F32)
        zsof[e] = r.astype(BF16)
        remote(zsof.at[e], zrof.at[e], zof_ss.at[0], zof_rs.at[0], to(z=(z + 2 + e) % Z)).start()
    sent_all(zrof, zof_ss.at[0])
    take(1)
    early_arrived(2, 0)
    early_over(2, 0).start()
    for e in range(NF):
        arrived(yrf.at[:, e], yf_rs.at[e])
        r = wvf[e, y].astype(F32)
        for d in range(Y - 1):
            r = r + yrf[d, e].astype(F32)
        zsf[e] = r.astype(BF16)
        remote(zsf.at[e], zrf.at[e], zf_ss.at[0], zf_rs.at[0], to(z=far_of(e))).start()
    sent_all(zrf, zf_ss.at[0])
    arrived(slg.at[0], slg_rs.at[RS[0]])
    arrived(wg.at[0], wo_rs.at[0])
    for part in range(2):
        arrived(wg.at[pl.ds(1, 6), 1 - yq, part], wy_rs.at[part])
    use(0)
    take(2)
    arrived(yrv, yv_rs.at[0])
    for e in range(NM):
        r = wvm[e, y].astype(F32)
        for d in range(Y - 1):
            r = r + yrv[d, e].astype(F32)
        zsv[e] = r.astype(BF16)
        remote(zsv.at[e], zrv.at[e], zv_ss.at[0], zv_rs.at[0], to(z=mid_of(e))).start()
    sent_all(zrv, zv_ss.at[0])
    near_sum(won, zron, zon_rs, yson, yron, yon_ss, yon_rs)
    take(3)
    use(1)
    use(2)
    use(3)
    near_sum(wvn, zrg, zg_rs, ysg, yrg, yg_ss, yg_rs)
    for slot in (4, 5):
        arrived(slg.at[slot, pl.ds(CH, 2 * CH)], slg_rs.at[RS[slot]])
        arrived(mr.at[slot - 1], mr_rs.at[slot - 4])
        for k in range(2):
            early_arrived(slot - 1, k)
        for q in range(NC):
            add(slot, q)

    order = [q for i in range(half) for q in (i, NC - 1 - i)]
    for k in range(2):
        early_arrived(5, k)
    for q in order:
        fwd[q].wait_recv()
        pfs[3, q] = pf(3, q)
        add(3, q)
    for q in order:
        pfs[3, q].wait_recv()
        add(6, q)
    ig[...] = acc[...].astype(BF16)

    arrived(zrof, zof_rs.at[0])
    arrived(yron, yon_rs.at[0])
    r = yson[y].astype(F32)
    for d in range(Y - 1):
        r = r + yron[d].astype(F32)
    for e in range(NO):
        r = r + zrof[e].astype(F32)
    og[...] = r
    arrived(tgz.at[pl.ds(0, Z - 1)], tz_rs.at[0])
    t = tgz[0].astype(F32)
    for zi in range(1, Z):
        t = t + tgz[zi].astype(F32)
    tg[...] = t[:K]
    ng[...] = t[K : K + 1]
    arrived(zrf, zf_rs.at[0])
    arrived(zrv, zv_rs.at[0])
    arrived(yrg, yg_rs.at[0])
    r = ysg[y].astype(F32)
    for got, count in ((yrg, Y - 1), (zrf, NF), (zrv, NM)):
        for e in range(count):
            r = r + got[e].astype(F32)
    vg[...] = r[:, :L]
    gg[...] = r[:, L:]

    for ref, ss in sent:
        arrived(ref, ss)

    @pl.when(jnp.logical_not(last))
    def _():
        halo_m.wait_send()

    @pl.when(jnp.logical_not(first))
    def _():
        halo_c.wait_send()


def write_out(*refs):
    half = len(refs) // 2
    for src, dst in zip(refs[:half], refs[half:]):
        dst[...] = src[...]


def shards(Z, Y, block_input, value_proj, gate_proj, conv_taps, norm_gain, out_proj, grad_output):
    rows, D = block_input.shape
    K = conv_taps.shape[0]
    C = value_proj.shape[1] * 8
    DB, RB, T = D // 8, D // (Z * Y), rows // S
    vm = pltpu.VMEM
    dma = pltpu.SemaphoreType.DMA
    hbm, vmem = pl.BlockSpec(memory_space=ANYWHERE), pl.BlockSpec(memory_space=pltpu.VMEM)
    near, wide = vm((S * NP, L), F32), vm((S * HP, L), F32)
    flat = vm((T, S, L), F32)
    halo = vm((PAD, L), F32)
    stat, stats = vm((2, S, L), F32), vm((7, 2, S, L), F32)
    scratch = [
        vm((rows, D), BF16), vm((rows, D), BF16), vm((D, 2 * L), BF16), vm((D, L), BF16), vm((7, 2, 2, DB // 4, 2 * L), BF16),
        near, near, near, wide, flat, flat, flat, flat, near, wide,
        near, near, vm((rows, 2 * L), BF16), vm((7, rows, 2 * L), BF16), vm((rows, DB), F32),
        vm((rows, 2 * L), BF16), vm((6, 2, rows // NC, 2 * L), BF16), near, vm((rows, L), BF16), vm((6, 2, rows // NC, L), BF16),
        halo, halo, halo, halo, vm((K, L), F32), vm((1, L), F32),
        vm((L, rows), BF16), vm((2 * L, rows), BF16),
        vm((NO, Y, RB, L), BF16), vm((NN + 1, Y, RB, L), BF16),
        vm((NF, Y, RB, 2 * L), BF16), vm((NM, Y, RB, 2 * L), BF16), vm((NN + 1, Y, RB, 2 * L), BF16),
        vm((Y - 1, NO, RB, L), BF16), vm((Y - 1, NF, RB, 2 * L), BF16), vm((Y - 1, NM, RB, 2 * L), BF16),
        vm((NO, RB, L), BF16), vm((NF, RB, 2 * L), BF16), vm((NM, RB, 2 * L), BF16),
        vm((NO, RB, L), BF16), vm((NN, Y, RB, L), BF16), vm((NF, RB, 2 * L), BF16), vm((NM, RB, 2 * L), BF16),
        vm((NN, Y, RB, 2 * L), BF16), vm((Y, RB, 2 * L), BF16), vm((Y - 1, RB, 2 * L), BF16),
        vm((Y, RB, L), BF16), vm((Y - 1, RB, L), BF16),
        stat, stats, stat, stats,
        halo, vm((Y, PAD, L), F32), vm((PAD, L), BF16), vm((Z, PAD, L), BF16),
        pltpu.SemaphoreType.REGULAR((6,)),
        dma((4,)), dma((4,)), dma((4,)), *[dma((1,)) for _ in range(2)], *[dma((2,)) for _ in range(6)],
        *[dma((1,)) for _ in range(4)], dma((2,)), dma((19,)), dma((2,)), dma((1,)), dma((12,)), *[dma((1,)) for _ in range(5)], dma((NF,)), *[dma((1,)) for _ in range(18)],
    ]
    shapes = (
        jax.ShapeDtypeStruct((rows, DB), BF16),
        jax.ShapeDtypeStruct((RB, L), F32),
        jax.ShapeDtypeStruct((RB, L), F32),
        jax.ShapeDtypeStruct((RB, L), F32),
        jax.ShapeDtypeStruct((K, L), F32),
        jax.ShapeDtypeStruct((1, L), F32),
    )
    norm_gain = norm_gain.reshape(1, L)
    block_input, value_proj, gate_proj, conv_taps, norm_gain, out_proj, grad_output = (
        pltpu.with_memory_space_constraint(a, pltpu.HBM)
        for a in (block_input, value_proj, gate_proj, conv_taps, norm_gain, out_proj, grad_output)
    )
    outs = pl.pallas_call(
        functools.partial(body, Z, Y, C, K),
        out_shape=shapes,
        in_specs=[hbm] * 7,
        out_specs=[vmem] * 6,
        scratch_shapes=scratch,
        compiler_params=pltpu.CompilerParams(
            collective_id=0, has_side_effects=True, vmem_limit_bytes=VMEM_LIMIT
        ),
        name="block_backward",
    )(block_input, value_proj, gate_proj, conv_taps, norm_gain, out_proj, grad_output)
    outs = pl.pallas_call(
        write_out,
        out_shape=shapes,
        in_specs=[vmem] * 6,
        out_specs=[vmem] * 6,
        compiler_params=pltpu.CompilerParams(vmem_limit_bytes=4 * 1024 * 1024),
        name="write_out",
    )(*outs)
    return (*outs[:5], outs[5].reshape(L))


def solution(mesh):
    tp = mesh.shape["tp"]
    Y = 4
    Z = mesh.shape["sp"] // Y
    finer = Mesh(mesh.devices.reshape(Z, Y, tp // 2, 2), ("z", "y", "x", "c"))
    sp, ch = ("z", "y"), ("x", "c")
    return jax.shard_map(
        functools.partial(shards, Z, Y),
        mesh=finer,
        in_specs=(P(sp, None), P(None, ch), P(None, ch), P(None, ch), P(ch), P(None, ch), P(sp, None)),
        out_specs=(P(sp, ch), P(sp, ch), P(sp, ch), P(sp, ch), P(None, ch), P(ch)),
        check_vma=False,
    )
```

```python
import functools

import jax
import jax.numpy as jnp
from jax import lax
from jax.experimental import pallas as pl
from jax.experimental.pallas import tpu as pltpu
from jax.sharding import Mesh
from jax.sharding import PartitionSpec as P

MESH = pl.DeviceIdType.MESH
F32 = jnp.float32
BF16 = jnp.bfloat16
norm_floor = 0.1
ANYWHERE = pltpu.HBM
VMEM_LIMIT = 40 * 1024 * 1024
L = 128
S = 8
J = 16
NP = 132
HP = 164
PAD = 32
NN = 2
FAR0, NF = 3, 3
NM = 2
NO = NF + NM
NC = 4
EARLY = (0, 3)


def dot_nn(a, b):
    return lax.dot_general(a, b, (((1,), (0,)), ((), ())), preferred_element_type=F32)


def dot_nt(a, b):
    return lax.dot_general(a, b, (((1,), (1,)), ((), ())), preferred_element_type=F32)


def body(
    Z, Y, C, K,
    x_hbm, vp_hbm, gp_hbm, taps_hbm, gain_hbm, op_hbm, g_hbm,
    ig, vg, gg, og, tg, ng,
    xv, gv, wvg, wo, wg, vbuf, sbuf, slope, hist, convp, nrm, nsl, inv, act, cs, vsf, gsf, sl, slg, acc,
    sqb, er, msf, msl, mr, tail, halo_in, halo_out, halo_back, taps, gain,
    actT, slT, wof, won, wvf, wvm, wvn, yrof, yrf, yrv, zsof, zsf, zsv, zrof, zron, zrf, zrv, zrg, ysg, yrg, yson, yron, sta, star, stb, stbr, tgs, tgy, tgzs, tgz,
    in_sem, l_sem, x_sem, g_sem, wo_ss, wo_rs, w_ss, w_rs, wy_ss, wy_rs, h_ss, h_rs, sa_ss, sa_rs, sb_ss, sb_rs, slg_ss, slg_rs, mr_rs, er_ss, er_rs,
    yof_ss, yof_rs, yon_ss, yon_rs, yf_ss, yf_rs, yv_ss, yv_rs, yg_ss, yg_rs, zof_ss, zof_rs, zon_ss, zon_rs, zf_ss, zf_rs, zv_ss, zv_rs, zg_ss, zg_rs,
    ty_ss, ty_rs, tz_ss, tz_rs,
):
    z, y, x, c = (lax.axis_index(a) for a in ("z", "y", "x", "c"))
    rows, D = xv.shape
    T = rows // S
    DB = D // 8
    DQ = DB // 4
    RB = D // (Z * Y)
    CH = rows // NC
    H = K - 1

    yn = (y + 1) % Y
    zn = (z + (y + 1) // Y) % Z
    yb = (y + Y - 1) % Y
    zb = (z + Z - 1 + (y + Y - 1) // Y) % Z
    first = (z + y) == 0
    last = (z * Y + y) == (Z * Y - 1)
    xp, xm = (x + 1) % 4, (x + 3) % 4
    xs = (x, x + 1 - 2 * (x % 2), (x + 2) % 4, 3 - x)
    cc = (c, 1 - c)

    def to(z=z, y=y, x=x, c=c):
        return {"z": z, "y": y, "x": x, "c": c}

    def remote(src, dst, ss, rs, dev):
        return pltpu.make_async_remote_copy(
            src_ref=src, dst_ref=dst, send_sem=ss, recv_sem=rs, device_id=dev, device_id_type=MESH
        )

    tp_peers = [to(x=xs[o // 2], c=cc[o % 2]) for o in range(1, 8)]
    y_peers = [to(y=(y + d) % Y) for d in range(1, Y)]
    z_peers = [to(z=(z + d) % Z) for d in range(1, Z)]
    nxt, prv = to(z=zn, y=yn), to(z=zb, y=yb)
    sent = []

    def arrived(ref, rs):
        pltpu.make_async_copy(ref, ref, rs).wait()

    def sent_all(ref, ss):
        sent.append((ref, ss))


    loads = [
        pltpu.make_async_copy(vp_hbm, wvg.at[:, pl.ds(0, L)], l_sem.at[0]),
        pltpu.make_async_copy(gp_hbm, wvg.at[:, pl.ds(L, L)], l_sem.at[0]),
        pltpu.make_async_copy(op_hbm, wo, l_sem.at[1]),
        pltpu.make_async_copy(taps_hbm, taps, l_sem.at[2]),
        pltpu.make_async_copy(gain_hbm, gain, l_sem.at[3]),
    ]
    loads[0].start()
    loads[1].start()
    XC = 4
    XR = rows // XC

    def x_load(i):
        at = pl.ds(pl.multiple_of(i * XR, XR), XR)
        return pltpu.make_async_copy(x_hbm.at[at], xv.at[at], x_sem.at[i])

    def g_load(i):
        at = pl.ds(pl.multiple_of(i * XR, XR), XR)
        return pltpu.make_async_copy(g_hbm.at[at], gv.at[at], g_sem.at[i])

    for i in (XC - 1, *range(XC - 1)):
        x_load(i).start()
    for cp in loads[2:]:
        cp.start()
    for i in range(XC):
        g_load(i).start()

    barrier = pltpu.get_barrier_semaphore()
    for dev in (*tp_peers, *y_peers):
        pl.semaphore_signal(barrier, inc=1, device_id=dev, device_id_type=MESH)
    below, above = z > 0, z < Z - 1
    into, out_of = (y == 0) & below, (y == Y - 1) & above
    for there, dev in (
        (below, to(z=(z + Z - 1) % Z)),
        (above, to(z=(z + 1) % Z)),
        (into, prv),
        (out_of, nxt),
    ):

        @pl.when(there)
        def _(dev=dev):
            pl.semaphore_signal(barrier, inc=1, device_id=dev, device_id_type=MESH)

    greeted = len(tp_peers) + len(y_peers) + sum(
        jnp.where(there, 1, 0) for there in (below, above, into, out_of)
    )

    def pass_on(k):
        n = 2**k
        for i, there, at in ((0, z + n < Z, (z + n) % Z), (1, z >= n, (z + Z - n) % Z)):

            @pl.when(there)
            def _(i=i, at=at):
                pl.semaphore_signal(in_sem.at[2 * k + i], inc=1, device_id=to(z=at), device_id_type=MESH)

    def heard(k):
        n = 2**k
        for i, there in ((0, z >= n), (1, z + n < Z)):

            @pl.when(there)
            def _(i=i):
                pl.semaphore_wait(in_sem.at[2 * k + i], 1)


    arrived(wvg, l_sem.at[0])

    right, left = to(x=xp), to(x=xm)
    partner = to(c=1 - c)

    def piece(ref, q):
        return ref.at[pl.ds(q * CH, CH)]

    def early_own(k):
        src = piece(sqb, EARLY[k])
        return [
            remote(src, er.at[0, k], er_ss.at[0], er_rs.at[k], right),
            remote(src, er.at[1, k], er_ss.at[0], er_rs.at[2 + k], left),
        ]

    def early_on(k):
        return remote(er.at[k, k], er.at[2, k], er_ss.at[0], er_rs.at[4 + k], (right, left)[k])

    def early_over(i, k):
        return remote(er.at[i, k], er.at[i + 3, k], er_ss.at[0], er_rs.at[6 + 2 * i + k], partner)

    def early_arrived(i, k):
        arrived(er.at[i, k], er_rs.at[2 * i + k])

    def x_step(i, end):
        x_load(i).wait()
        res = dot_nn(xv[pl.ds(pl.multiple_of(i * XR, XR), XR), :], wvg[...])
        v = res[:, :L]
        s = jax.nn.sigmoid(res[:, L:])
        m = (v * s).astype(BF16).astype(F32)
        for h in range(XR // T):
            n = i * (XR // T) + h
            part = slice(h * T, (h + 1) * T)
            vbuf[pl.ds(n * NP, T), :] = v[part]
            sbuf[pl.ds(n * NP, T), :] = s[part]
            at = pl.ds(pl.multiple_of(n * T, T), T)
            sqb[at, pl.ds(0, L)] = s[part].astype(BF16)
            sqb[at, pl.ds(L, L)] = (v[part] * s[part] * (1.0 - s[part])).astype(BF16)
            hist[pl.ds(n * HP + PAD, T), :] = m[part]
            if end and h == XR // T - 1:
                tail[...] = m[XR - PAD :]
            else:
                hist[pl.ds((n + 1) * HP, PAD), :] = m[(h + 1) * T - PAD : (h + 1) * T]

    x_step(XC - 1, True)

    def x_loop(i, carry):
        x_step(i, False)
        return carry

    pl.semaphore_wait(barrier, greeted)
    halo_m = remote(tail, halo_in, h_ss.at[0], h_rs.at[0], nxt)

    @pl.when(jnp.logical_not(last))
    def _():
        halo_m.start()

    pass_on(0)

    yq = y % 2
    y_pair = to(y=y + 1 - 2 * yq)

    def w_start(part):
        for o in range(2, 8):
            row = (xs[o // 2] * 2 + cc[o % 2]) * DB + (2 * yq + part) * DQ
            at = pl.ds(pl.multiple_of(row, DQ), DQ)
            remote(
                wvg.at[at], wg.at[o - 1, yq, part], w_ss.at[part], w_rs.at[part], tp_peers[o - 1]
            ).start()
        sent_all(wg.at[pl.ds(1, 6), yq, part], w_ss.at[part])

    def w_on(part):
        at = wg.at[pl.ds(1, 6), yq, part]
        arrived(at, w_rs.at[part])
        remote(at, at, wy_ss.at[part], wy_rs.at[part], y_pair).start()
        sent_all(at, wy_ss.at[part])

    w_start(0)
    for i in range(4):
        at = pl.ds(pl.multiple_of((xs[0] * 2 + cc[1]) * DB + i * DQ, DQ), DQ)
        remote(wvg.at[at], wg.at[0, i // 2, i % 2], wo_ss.at[0], wo_rs.at[0], tp_peers[0]).start()
    sent_all(wg.at[0], wo_ss.at[0])

    lax.fori_loop(0, XC - 1, x_loop, 0)

    for cp in loads[2:]:
        cp.wait()

    lane = lax.broadcasted_iota(jnp.int32, (S, L), 1)
    zero = jnp.zeros((S, L), F32)

    def near(ref, t):
        return ref[pl.ds(t, S, stride=NP), :]

    def wide(ref, t):
        return ref[pl.ds(t, S, stride=HP), :]

    def spread(stat, t):
        return jnp.sum(jnp.where(lane == t, stat, 0.0), axis=1, keepdims=True)

    def tap(k):
        return taps[pl.ds(k, 1), :]

    def conv_block(b, carry):
        s1, s2 = carry
        t0 = b * J
        r = [zero] * J
        for i in range(J + H):
            m = wide(hist, t0 + (PAD - H) + i)
            for j in range(J):
                k = H + j - i
                if 0 <= k < K:
                    r[j] = r[j] + tap(k) * m
        for j in range(J):
            convp[t0 + j] = r[j]
            s1 = jnp.where(lane == t0 + j, jnp.sum(r[j], axis=1, keepdims=True), s1)
            s2 = jnp.where(lane == t0 + j, jnp.sum(r[j] * r[j], axis=1, keepdims=True), s2)
        return s1, s2

    def exchange(own, got, ss, rs):
        copies = [remote(own, got.at[i], ss.at[0], rs.at[0], tp_peers[i]) for i in range(7)]
        for cp in copies:
            cp.start()
        sent_all(got, ss.at[0])

    def total(own, got, i):
        r = own[i]
        for p in range(7):
            r = r + got[p, i]
        return r * (1.0 / C)

    near_end = -(-H // J)
    s1, s2 = lax.fori_loop(near_end, T // J, conv_block, (zero, zero))

    @pl.when(first)
    def _():
        hist[pl.ds(0, PAD), :] = jnp.zeros((PAD, L), F32)

    @pl.when(jnp.logical_not(first))
    def _():
        halo_m.wait_recv()
        hist[pl.ds(0, PAD), :] = halo_in[...]

    s1, s2 = lax.fori_loop(0, near_end, conv_block, (s1, s2))
    sta[0] = s1
    sta[1] = s2
    exchange(sta, star, sa_ss, sa_rs)
    w_start(1)
    for cp in early_own(1):
        cp.start()

    def g_loop(i, carry):
        g_load(i).wait()
        r = dot_nn(gv[pl.ds(pl.multiple_of(i * XR, XR), XR), :], wo[...])
        for h in range(XR // T):
            slope[pl.ds((i * (XR // T) + h) * NP, T), :] = r[h * T : (h + 1) * T]
        return carry

    lax.fori_loop(0, XC, g_loop, 0)

    heard(0)
    pass_on(1)

    w_on(0)

    arrived(star, sa_rs.at[0])
    center = total(sta, star, 0)
    inverse = lax.rsqrt(total(sta, star, 1) - center * center + norm_floor)
    gains = gain[...]

    def norm_block(b, carry):
        gsum, s1, s2 = carry
        t0 = b * J
        for j in range(J):
            t = t0 + j
            iv = jnp.broadcast_to(spread(inverse, t), (S, L))
            n = (convp[t] - spread(center, t)) * iv
            sc = n * gains
            sq = jax.nn.sigmoid(sc)
            act[pl.ds(t, S, stride=NP), :] = sc * sq
            ps = near(slope, t) * sq * (1.0 + sc * (1.0 - sq))
            gsum = gsum + ps * n
            ns = ps * gains
            inv[t] = iv
            nrm[t] = n
            nsl[t] = ns
            s1 = jnp.where(lane == t, jnp.sum(ns, axis=1, keepdims=True), s1)
            s2 = jnp.where(lane == t, jnp.sum(ns * n, axis=1, keepdims=True), s2)
        return gsum, s1, s2

    gsum, s1, s2 = lax.fori_loop(0, T // J, norm_block, (zero, zero, zero))
    stb[0] = s1
    stb[1] = s2
    exchange(stb, stbr, sb_ss, sb_rs)
    heard(1)
    pass_on(2)
    for cp in early_own(0):
        cp.start()
    w_on(1)

    def flip(src, dst, row0):
        def step(n, carry):
            dst[pl.ds(row0, L), pl.ds(pl.multiple_of(n * T, T), T)] = src[pl.ds(n * NP, T), :].T.astype(BF16)
            return carry

        lax.fori_loop(0, S, step, 0)

    flip(act, actT, 0)

    def weight_block(left, right, zi, put):
        at = pl.ds(pl.multiple_of(zi * (D // Z), D // Z), D // Z)
        r = dot_nn(left[...], right[:, at]).T.astype(BF16)
        for yi in range(Y):
            put(yi, r[yi * RB : (yi + 1) * RB])

    def y_send(src, dst, ss, rs):
        for d in range(1, Y):
            remote(src.at[:, (y + d) % Y], dst.at[d - 1], ss.at[0], rs.at[0], y_peers[d - 1]).start()
        sent_all(dst, ss.at[0])

    def near_of(e):
        return (z + Z + 1 - 2 * e) % Z

    def mid_of(e):
        return (z + 2 + (Z - 4) * e) % Z

    def out_put(dst, e):
        def put(yi, r):
            dst[e, yi] = r

        return put

    def out_near_loop(e, carry):
        weight_block(actT, gv, near_of(e), out_put(won, e))
        return carry

    def out_far_loop(e, carry):
        weight_block(actT, gv, (z + 2 + e) % Z, out_put(wof, e))
        return carry

    lax.fori_loop(0, NO, out_far_loop, 0)
    weight_block(actT, gv, z, out_put(won, NN))
    lax.fori_loop(0, NN, out_near_loop, 0)

    for i in range(2):
        early_arrived(i, 1)
        early_over(i, 1).start()
    early_on(1).start()

    arrived(stbr, sb_rs.at[0])
    slope_sum = total(stb, stbr, 0)
    cross_sum = total(stb, stbr, 1)

    def cs_block(b, carry):
        t0 = b * J
        for j in range(J):
            t = t0 + j
            cs[pl.ds(t, S, stride=HP), :] = inv[t] * (
                nsl[t] - spread(slope_sum, t) - nrm[t] * spread(cross_sum, t)
            )
        return carry

    lax.fori_loop(0, PAD // J, cs_block, 0)
    halo_out[...] = cs[pl.ds(0, PAD), :]
    halo_c = remote(halo_out, halo_back, h_ss.at[1], h_rs.at[1], prv)

    @pl.when(jnp.logical_not(first))
    def _():
        halo_c.start()

    y_send(wof, yrof, yof_ss, yof_rs)
    for n in range(S - 1):
        cs[pl.ds(n * HP + T, PAD), :] = cs[pl.ds((n + 1) * HP, PAD), :]
    lax.fori_loop(PAD // J, T // J, cs_block, 0)

    def slope_block(b, carry):
        t0 = b * J
        r = [zero] * J
        for i in range(J + H):
            f = wide(cs, t0 + i)
            for j in range(J):
                k = i - j
                if 0 <= k < K:
                    r[j] = r[j] + tap(k) * f
        for j in range(J):
            t = t0 + j
            s = near(sbuf, t)
            msf[pl.ds(t, S, stride=NP), :] = r[j]
            rs = r[j] * s
            vsf[pl.ds(t, S, stride=NP), :] = rs
            gsf[pl.ds(t, S, stride=NP), :] = rs * near(vbuf, t) * (1.0 - s)
        return carry

    free = (T - H) // J
    lax.fori_loop(0, free, slope_block, 0)

    def tap_block(b, sums):
        sums = list(sums)
        t0 = b * 8
        e = [wide(cs, t0 + j) for j in range(8)]
        for i in range(8 + H):
            m = wide(hist, t0 + (PAD - H) + i)
            for j in range(8):
                k = H + j - i
                if 0 <= k < K:
                    sums[k] = sums[k] + e[j] * m
        return tuple(sums)

    for i in range(2):
        early_arrived(i, 0)
        early_over(i, 0).start()
    early_on(0).start()
    sent_all(er, er_ss.at[0])

    sums = lax.fori_loop(0, T // 8, tap_block, tuple(zero for _ in range(K)))
    for k in range(K):
        tgs[pl.ds(k, 1), :] = jnp.sum(sums[k], axis=0, keepdims=True)
    tgs[pl.ds(K, 1), :] = jnp.sum(gsum, axis=0, keepdims=True)
    for d in range(1, Y):
        remote(tgs, tgy.at[y], ty_ss.at[0], ty_rs.at[0], y_peers[d - 1]).start()
    sent_all(tgy.at[pl.ds(0, Y - 1)], ty_ss.at[0])
    tgy[y] = tgs[...]


    @pl.when(last)
    def _():
        cs[pl.ds((S - 1) * HP + T, PAD), :] = jnp.zeros((PAD, L), F32)

    @pl.when(jnp.logical_not(last))
    def _():
        halo_c.wait_recv()
        cs[pl.ds((S - 1) * HP + T, PAD), :] = halo_back[...]

    lax.fori_loop(free, T // J, slope_block, 0)

    def to_bf16(n, carry):
        at = pl.ds(pl.multiple_of(n * T, T), T)
        msl[at, :] = msf[pl.ds(n * NP, T), :].astype(BF16)
        sl[at, pl.ds(0, L)] = vsf[pl.ds(n * NP, T), :].astype(BF16)
        sl[at, pl.ds(L, L)] = gsf[pl.ds(n * NP, T), :].astype(BF16)
        return carry

    lax.fori_loop(0, S, to_bf16, 0)

    RS = (0, 1, 5, 9, 13, 14, 15)

    def held(slot, q):
        return mr.at[slot - 1, EARLY.index(q)] if q in EARLY else piece(slg.at[slot], q)

    def pass_slope(src, slot, q, sem, dev):
        return remote(src, held(slot, q), slg_ss.at[1 if q in EARLY else 0], sem, dev)

    def own_copy(slot, q, dev):
        return pass_slope(piece(msl if q in EARLY else sl, q), slot, q, slg_rs.at[RS[slot] + q], dev)

    up = [own_copy(1, q, right) for q in range(NC)]
    down = [own_copy(2, q, left) for q in range(NC)]
    over = [remote(piece(sl, q), piece(slg.at[0], q), slg_ss.at[0], slg_rs.at[0], partner) for q in range(NC)]
    half = NC // 2
    for i in range(NC):
        up[i].start()
        down[NC - 1 - i].start()
    for i in range(NC):
        over[i].start()
    sent_all(slg.at[pl.ds(0, 4)], slg_ss.at[0])
    sent_all(mr, slg_ss.at[1])

    heard(2)
    for e in range(NN):
        remote(won.at[e], zron.at[e], zon_ss.at[0], zon_rs.at[0], to(z=near_of(e))).start()
    sent_all(zron, zon_ss.at[0])
    diagonal = (
        lax.broadcasted_iota(jnp.int32, (2 * L, 2 * L), 0) == lax.broadcasted_iota(jnp.int32, (2 * L, 2 * L), 1)
    ).astype(F32).astype(BF16)
    slT[...] = dot_nt(diagonal, sl[...]).astype(BF16)

    def far_of(e):
        return (z + FAR0 + 1 - e % 2 + e // 2) % Z

    def far_loop(e, carry):
        def put(yi, r):
            wvf[e, yi] = r

        weight_block(slT, xv, far_of(e), put)
        for d in range(1, Y):
            remote(
                wvf.at[e, (y + d) % Y], yrf.at[d - 1, e], yf_ss.at[0], yf_rs.at[e], y_peers[d - 1]
            ).start()
        return carry

    def mid_loop(e, carry):
        weight_block(slT, xv, mid_of(e), out_put(wvm, e))
        return carry

    def near_send(e):
        return remote(wvn.at[e], zrg.at[e], zg_ss.at[0], zg_rs.at[0], to(z=near_of(e)))

    def near_loop(e, carry):
        weight_block(slT, xv, near_of(e), out_put(wvn, e))
        near_send(e).start()
        return carry

    lax.fori_loop(0, NF, far_loop, 0)
    sent_all(yrf, yf_ss.at[0])
    lax.fori_loop(0, NN, near_loop, 0)
    sent_all(zrg, zg_ss.at[0])
    lax.fori_loop(0, NM, mid_loop, 0)
    y_send(wvm, yrv, yv_ss, yv_rs)
    weight_block(slT, xv, z, out_put(wvn, NN))

    def weights_from(slot):
        core = 1 if slot == 0 or slot > 3 else 0
        base = slot if slot <= 3 else slot - 3
        if base == 0:
            return wg[0].reshape(DB, 2 * L)
        if base == 3:
            return wg[3 + core].reshape(DB, 2 * L)
        way = 3 - 2 * (x % 2) if base == 1 else 1 + 2 * (x % 2)
        return wg[2 * way + core - 1].reshape(DB, 2 * L)

    at = pl.ds(pl.multiple_of((x * 2 + c) * DB, DB), DB)
    acc[...] = dot_nt(sl[...], wvg[at, :])

    def add(slot, q):
        at = pl.ds(q * CH, CH)
        if slot and q in EARLY:
            k = EARLY.index(q)
            m = mr[slot - 1, k].astype(F32)
            f = er[slot - 1, k].astype(F32)
            block = jnp.concatenate([m * f[:, :L], m * f[:, L:]], axis=1).astype(BF16)
        else:
            block = slg[slot, at, :]
        acc[at, :] += dot_nt(block, weights_from(slot))

    def pf(slot, q):
        if slot == 3:
            sem = slg_rs.at[RS[6] + q]
        else:
            sem = mr_rs.at[slot - 1] if q in EARLY else slg_rs.at[RS[slot + 3]]
        cp = pass_slope(held(slot, q), slot + 3, q, sem, partner)
        cp.start()
        return cp

    def near_sum(own, got, z_rs, ys, yr, y_ss, y_rs):
        arrived(got, z_rs.at[0])
        for yi in range(Y):
            r = own[NN, yi].astype(F32)
            for e in range(NN):
                r = r + got[e, yi].astype(F32)
            ys[yi] = r.astype(BF16)
        for d in range(1, Y):
            remote(ys.at[(y + d) % Y], yr.at[d - 1], y_ss.at[0], y_rs.at[0], y_peers[d - 1]).start()
        sent_all(yr, y_ss.at[0])

    fwd = {}
    pfs = {}

    def take(i):
        for slot, q, copies, way in ((1, i, up, right), (2, NC - 1 - i, down, left)):
            copies[q].wait_recv()
            if i < half:
                fwd[q] = pass_slope(held(slot, q), 3, q, slg_rs.at[RS[3] + q], way)
                fwd[q].start()
            pfs[slot, q] = pf(slot, q)

    def use(i):
        add(0, i)
        add(1, i)
        add(2, NC - 1 - i)

    take(0)
    early_arrived(2, 1)
    early_over(2, 1).start()
    arrived(tgy.at[pl.ds(0, Y - 1)], ty_rs.at[0])
    t = tgy[0]
    for yi in range(1, Y):
        t = t + tgy[yi]
    tgzs[...] = t.astype(BF16)
    tgz[z] = t.astype(BF16)
    for d in range(1, Z):
        remote(tgzs, tgz.at[z], tz_ss.at[0], tz_rs.at[0], z_peers[d - 1]).start()
    sent_all(tgz.at[pl.ds(0, Z - 1)], tz_ss.at[0])
    arrived(yrof, yof_rs.at[0])
    for e in range(NO):
        r = wof[e, y].astype(F32)
        for d in range(Y - 1):
            r = r + yrof[d, e].astype(F32)
        zsof[e] = r.astype(BF16)
        remote(zsof.at[e], zrof.at[e], zof_ss.at[0], zof_rs.at[0], to(z=(z + 2 + e) % Z)).start()
    sent_all(zrof, zof_ss.at[0])
    take(1)
    early_arrived(2, 0)
    early_over(2, 0).start()
    for e in range(NF):
        arrived(yrf.at[:, e], yf_rs.at[e])
        r = wvf[e, y].astype(F32)
        for d in range(Y - 1):
            r = r + yrf[d, e].astype(F32)
        zsf[e] = r.astype(BF16)
        remote(zsf.at[e], zrf.at[e], zf_ss.at[0], zf_rs.at[0], to(z=far_of(e))).start()
    sent_all(zrf, zf_ss.at[0])
    arrived(slg.at[0], slg_rs.at[RS[0]])
    arrived(wg.at[0], wo_rs.at[0])
    for part in range(2):
        arrived(wg.at[pl.ds(1, 6), 1 - yq, part], wy_rs.at[part])
    use(0)
    take(2)
    arrived(yrv, yv_rs.at[0])
    for e in range(NM):
        r = wvm[e, y].astype(F32)
        for d in range(Y - 1):
            r = r + yrv[d, e].astype(F32)
        zsv[e] = r.astype(BF16)
        remote(zsv.at[e], zrv.at[e], zv_ss.at[0], zv_rs.at[0], to(z=mid_of(e))).start()
    sent_all(zrv, zv_ss.at[0])
    near_sum(won, zron, zon_rs, yson, yron, yon_ss, yon_rs)
    take(3)
    use(1)
    use(2)
    use(3)
    near_sum(wvn, zrg, zg_rs, ysg, yrg, yg_ss, yg_rs)
    for slot in (4, 5):
        arrived(slg.at[slot, pl.ds(CH, 2 * CH)], slg_rs.at[RS[slot]])
        arrived(mr.at[slot - 1], mr_rs.at[slot - 4])
        for k in range(2):
            early_arrived(slot - 1, k)
        for q in range(NC):
            add(slot, q)

    order = [q for i in range(half) for q in (i, NC - 1 - i)]
    for k in range(2):
        early_arrived(5, k)
    for q in order:
        fwd[q].wait_recv()
        pfs[3, q] = pf(3, q)
        add(3, q)
    for q in order:
        pfs[3, q].wait_recv()
        add(6, q)
    ig[...] = acc[...].astype(BF16)

    arrived(zrof, zof_rs.at[0])
    arrived(yron, yon_rs.at[0])
    r = yson[y].astype(F32)
    for d in range(Y - 1):
        r = r + yron[d].astype(F32)
    for e in range(NO):
        r = r + zrof[e].astype(F32)
    og[...] = r
    arrived(tgz.at[pl.ds(0, Z - 1)], tz_rs.at[0])
    t = tgz[0].astype(F32)
    for zi in range(1, Z):
        t = t + tgz[zi].astype(F32)
    tg[...] = t[:K]
    ng[...] = t[K : K + 1]
    arrived(zrf, zf_rs.at[0])
    arrived(zrv, zv_rs.at[0])
    arrived(yrg, yg_rs.at[0])
    r = ysg[y].astype(F32)
    for got, count in ((yrg, Y - 1), (zrf, NF), (zrv, NM)):
        for e in range(count):
            r = r + got[e].astype(F32)
    vg[...] = r[:, :L]
    gg[...] = r[:, L:]

    for ref, ss in sent:
        arrived(ref, ss)

    @pl.when(jnp.logical_not(last))
    def _():
        halo_m.wait_send()

    @pl.when(jnp.logical_not(first))
    def _():
        halo_c.wait_send()


def write_out(*refs):
    half = len(refs) // 2
    for src, dst in zip(refs[:half], refs[half:]):
        dst[...] = src[...]


def shards(Z, Y, block_input, value_proj, gate_proj, conv_taps, norm_gain, out_proj, grad_output):
    rows, D = block_input.shape
    K = conv_taps.shape[0]
    C = value_proj.shape[1] * 8
    DB, RB, T = D // 8, D // (Z * Y), rows // S
    vm = pltpu.VMEM
    dma = pltpu.SemaphoreType.DMA
    hbm, vmem = pl.BlockSpec(memory_space=ANYWHERE), pl.BlockSpec(memory_space=pltpu.VMEM)
    near, wide = vm((S * NP + T, L), F32), vm((S * HP + T + PAD, L), F32)
    flat = vm((T, S, L), F32)
    halo = vm((PAD, L), F32)
    stat, stats = vm((2, S, L), F32), vm((7, 2, S, L), F32)
    scratch = [
        vm((rows, D), BF16), vm((rows, D), BF16), vm((D, 2 * L), BF16), vm((D, L), BF16), vm((7, 2, 2, DB // 4, 2 * L), BF16),
        near, near, near, wide, flat, flat, flat, flat, near, wide,
        near, near, vm((rows, 2 * L), BF16), vm((7, rows, 2 * L), BF16), vm((rows, DB), F32),
        vm((rows, 2 * L), BF16), vm((6, 2, rows // NC, 2 * L), BF16), near, vm((rows, L), BF16), vm((6, 2, rows // NC, L), BF16),
        halo, halo, halo, halo, vm((K, L), F32), vm((1, L), F32),
        vm((L, rows), BF16), vm((2 * L, rows), BF16),
        vm((NO, Y, RB, L), BF16), vm((NN + 1, Y, RB, L), BF16),
        vm((NF, Y, RB, 2 * L), BF16), vm((NM, Y, RB, 2 * L), BF16), vm((NN + 1, Y, RB, 2 * L), BF16),
        vm((Y - 1, NO, RB, L), BF16), vm((Y - 1, NF, RB, 2 * L), BF16), vm((Y - 1, NM, RB, 2 * L), BF16),
        vm((NO, RB, L), BF16), vm((NF, RB, 2 * L), BF16), vm((NM, RB, 2 * L), BF16),
        vm((NO, RB, L), BF16), vm((NN, Y, RB, L), BF16), vm((NF, RB, 2 * L), BF16), vm((NM, RB, 2 * L), BF16),
        vm((NN, Y, RB, 2 * L), BF16), vm((Y, RB, 2 * L), BF16), vm((Y - 1, RB, 2 * L), BF16),
        vm((Y, RB, L), BF16), vm((Y - 1, RB, L), BF16),
        stat, stats, stat, stats,
        halo, vm((Y, PAD, L), F32), vm((PAD, L), BF16), vm((Z, PAD, L), BF16),
        pltpu.SemaphoreType.REGULAR((6,)),
        dma((4,)), dma((4,)), dma((4,)), *[dma((1,)) for _ in range(2)], *[dma((2,)) for _ in range(6)],
        *[dma((1,)) for _ in range(4)], dma((2,)), dma((19,)), dma((2,)), dma((1,)), dma((12,)), *[dma((1,)) for _ in range(5)], dma((NF,)), *[dma((1,)) for _ in range(18)],
    ]
    shapes = (
        jax.ShapeDtypeStruct((rows, DB), BF16),
        jax.ShapeDtypeStruct((RB, L), F32),
        jax.ShapeDtypeStruct((RB, L), F32),
        jax.ShapeDtypeStruct((RB, L), F32),
        jax.ShapeDtypeStruct((K, L), F32),
        jax.ShapeDtypeStruct((1, L), F32),
    )
    norm_gain = norm_gain.reshape(1, L)
    block_input, value_proj, gate_proj, conv_taps, norm_gain, out_proj, grad_output = (
        pltpu.with_memory_space_constraint(a, pltpu.HBM)
        for a in (block_input, value_proj, gate_proj, conv_taps, norm_gain, out_proj, grad_output)
    )
    outs = pl.pallas_call(
        functools.partial(body, Z, Y, C, K),
        out_shape=shapes,
        in_specs=[hbm] * 7,
        out_specs=[vmem] * 6,
        scratch_shapes=scratch,
        compiler_params=pltpu.CompilerParams(
            collective_id=0, has_side_effects=True, vmem_limit_bytes=VMEM_LIMIT
        ),
        name="block_backward",
    )(block_input, value_proj, gate_proj, conv_taps, norm_gain, out_proj, grad_output)
    outs = pl.pallas_call(
        write_out,
        out_shape=shapes,
        in_specs=[vmem] * 6,
        out_specs=[vmem] * 6,
        compiler_params=pltpu.CompilerParams(vmem_limit_bytes=4 * 1024 * 1024),
        name="write_out",
    )(*outs)
    return (*outs[:5], outs[5].reshape(L))


def solution(mesh):
    tp = mesh.shape["tp"]
    Y = 4
    Z = mesh.shape["sp"] // Y
    finer = Mesh(mesh.devices.reshape(Z, Y, tp // 2, 2), ("z", "y", "x", "c"))
    sp, ch = ("z", "y"), ("x", "c")
    return jax.shard_map(
        functools.partial(shards, Z, Y),
        mesh=finer,
        in_specs=(P(sp, None), P(None, ch), P(None, ch), P(None, ch), P(ch), P(None, ch), P(sp, None)),
        out_specs=(P(sp, ch), P(sp, ch), P(sp, ch), P(sp, ch), P(None, ch), P(ch)),
        check_vma=False,
    )
```
